768 devices in a mesh: ep: 24 (over z, core), tp: 32 (over y, x).
Axes of the slice: x: 4, y: 8, z: 12, core: 2. Of those that a mesh axis runs over, the one named last changes fastest.
Arguments:
- tokens: bfloat16 [3072, 2048], P('ep', 'tp'), may hold values from -6 to 6
- out_grad: bfloat16 [3072, 2048], P('ep', 'tp'), may hold values from -6 to 6
- routes: int32 [3072, 2], P('ep'), may hold values from 0 to 23, all different within a row; in each aligned block of 128 rows (0 to 127, 128 to 255, ...) at most 16 rows name the same one
- gates: float32 [3072, 2], P('ep'), may hold values from 0.1 to 0.9
- gate_weight: bfloat16 [24, 2048, 5632], P('ep', None, 'tp'), may hold values from -0.125 to 0.125
- up_weight: bfloat16 [24, 2048, 5632], P('ep', None, 'tp'), may hold values from -0.125 to 0.125
- down_weight: bfloat16 [24, 5632, 2048], P('ep', 'tp'), may hold values from -0.078125 to 0.078125
Outputs:
- tokens_grad: bfloat16 [3072, 2048], P('ep', 'tp')
- gates_grad: float32 [3072, 2], P(('ep', 'tp'))
- gate_weight_grad: bfloat16 [24, 2048, 5632], P('ep', None, 'tp')
- up_weight_grad: bfloat16 [24, 2048, 5632], P('ep', None, 'tp')
- down_weight_grad: bfloat16 [24, 5632, 2048], P('ep', 'tp')
The draws below stay inside these ranges and needn't reach their ends.
Inputs may be any that keep to these rules, and one draw needn't show every extreme that they name: `routes`: the 2 experts of a token differ. In each aligned block of 128 rows (the tokens of one index of ep) no expert is named by more than 16 rows, a bound that some block reaches.
All inputs are finite; a program needn't handle non-finite values.
Results may differ from the reference program's by a relative error of at most 0.029.
Values may be sent and summed in bfloat16 or wider, within the bound.
No kernel may reach another device: no remote copies, remote signals or barrier semaphores. Data moves between devices by JAX's collectives and lax.ppermute only.
A program may use at most 64 MiB of HBM per device.

```python
import math
import jax
import jax.numpy as jnp
import numpy as np
from jax import lax

D = 2048
FF = 5632
TOPK = 2
TOK_DEV = 128
EXPERTS = 24
CAP = 16
TOKENS = 3072
N_EP = 24
N_TP = 32


def block_scale(stream_key, dims, split, least, top_value):
    gain = 1.0
    for dim, parts in split:
        steps = jax.random.uniform(jax.random.fold_in(jax.random.fold_in(stream_key, 6), dim), (parts,), jnp.float32, least / len(split), top_value / len(split))
        gain = gain * jnp.repeat(jnp.exp(steps), dims[dim] // parts).reshape((-1,) + (1,) * (len(dims) - 1 - dim))
    return gain


def routed_block(own_key, own, number, rows, count, top, reach, slope):
    ranking = jax.random.permutation(own_key, count)
    crowded, ordinary = portions_of(count, rows * top, reach, slope, True), portions_of(count, rows * top, reach, slope, False)
    places = jnp.arange(count)

    def named(tallies, rotation):
        used = int((tallies > 0).sum())
        fixed = max(1, used // 4)
        moved = fixed + (places - fixed + rotation * (used - fixed)) % max(1, count - fixed)
        return jnp.zeros((count,), jnp.int32).at[ranking[jnp.where(places < fixed, places, moved)]].set(jnp.asarray(tallies, jnp.int32))

    tallies = jnp.where(number % 4 == 0, named(crowded, number // 4), named(ordinary, number - number // 4 - 1))
    mixed = jax.random.permutation(jax.random.fold_in(own, 3), count)
    source_of, taker = mixed[0:count // 2 * 2:2], mixed[1:count // 2 * 2:2]
    room = jnp.minimum(tallies[source_of] - 1, reach - tallies[taker]) // 2
    room = jnp.where((source_of == ranking[0]) | (taker == ranking[0]) | (tallies[taker] == 0), 0, jnp.maximum(room, 0))
    moved = jax.random.randint(jax.random.fold_in(own, 4), (count // 2,), 0, 1 << 20) % (room + 1)
    tallies = tallies.at[source_of].add(-moved).at[taker].add(moved)
    items = jnp.searchsorted(jnp.cumsum(tallies), jnp.arange(rows * top), side="right").astype(jnp.int32)
    grid = items.reshape(top, rows).T
    grid = grid[jax.random.permutation(jax.random.fold_in(own, 1), rows)]
    rotation = jax.random.randint(jax.random.fold_in(own, 2), (rows, 1), 0, top)
    return jnp.take_along_axis(grid, (jnp.arange(top)[None, :] + rotation) % top, axis=1)


def portions_of(count, total, bound, slope, full):
    portions = [(1 << 20) // math.isqrt(rank ** slope) + 1 for rank in range(1, count + 1)]
    largest = bound if full else min(bound, max(-(-total // count), total * portions[0] // sum(portions)))
    least = 1 if total - largest >= count - 1 else 0
    holding, surplus = [largest] + [least] * (count - 1), total - largest - least * (count - 1)
    while surplus > 0:
        free = [i for i in range(1, count) if holding[i] < largest] or [i for i in range(1, count) if holding[i] < bound]
        pool, left = sum([portions[i] for i in free]), surplus
        for i in free:
            addition = min(bound - holding[i], max(1, left * portions[i] // pool), surplus)
            holding[i] = holding[i] + addition
            surplus = surplus - addition
    return np.array(holding)


def scatter_about(stream_key, extent, deviation, most, cuts=(), held_as=jnp.bfloat16):
    loudness = block_scale(stream_key, extent, cuts, -0.22, 0.18) if cuts else 1.0
    entries = jax.random.normal(stream_key, extent, jnp.float32) * deviation * loudness
    return jnp.minimum(jnp.maximum(entries, -most), most).astype(held_as)


def setup_inputs(seed: int = 0) -> dict:
    arg_keys = jax.random.split(jax.random.key(seed), 8)
    tokens = scatter_about(arg_keys[0], (TOKENS, D), 1.0, 6.0, ((0, 24), (1, 32)))
    out_grad = scatter_about(arg_keys[1], (TOKENS, D), 1.0, 6.0, ((0, 24), (1, 32)))
    routes_keys = jax.random.split(jax.random.fold_in(arg_keys[2], 1), TOKENS // TOK_DEV)
    routes_turns = jax.random.permutation(jax.random.fold_in(arg_keys[2], 3), TOKENS // TOK_DEV)
    routes = jax.vmap(lambda own, number: routed_block(jax.random.fold_in(arg_keys[2], 2), own, number, TOK_DEV, EXPERTS, TOPK, CAP, 2))(routes_keys, routes_turns).reshape((TOKENS, TOPK))
    gates = jnp.clip(0.1 + 0.79999997 * jax.random.uniform(arg_keys[3], (TOKENS, TOPK), jnp.float32) ** block_scale(arg_keys[3], (TOKENS, TOPK), ((0, 24),), -0.2, 0.2), 0.1, 0.9)
    gate_weight = scatter_about(arg_keys[4], (EXPERTS, D, FF), D ** -0.5, 0.125, ((0, 24), (2, 32)))
    up_weight = scatter_about(arg_keys[5], (EXPERTS, D, FF), D ** -0.5, 0.125, ((0, 24), (2, 32)))
    down_weight = scatter_about(arg_keys[6], (EXPERTS, FF, D), FF ** -0.5, 0.078125, ((0, 24), (1, 32)))
    return {"tokens": tokens, "out_grad": out_grad, "routes": routes, "gates": gates, "gate_weight": gate_weight, "up_weight": up_weight, "down_weight": down_weight}


def expert_grads(rows, cotan, w_gate, w_up, w_down):
    pre_gate = jnp.dot(rows, w_gate, preferred_element_type=jnp.float32)
    pre_up = jnp.dot(rows, w_up, preferred_element_type=jnp.float32)
    activated = jax.nn.silu(pre_gate)
    hidden = (activated * pre_up).astype(jnp.bfloat16)
    hid_grad = jnp.dot(cotan, w_down.T, preferred_element_type=jnp.float32)
    sigmoid_gate = jax.nn.sigmoid(pre_gate)
    gate_part = (hid_grad * pre_up * sigmoid_gate * (1.0 + pre_gate * (1.0 - sigmoid_gate))).astype(jnp.bfloat16)
    up_part = (hid_grad * activated).astype(jnp.bfloat16)
    slot_dots = jnp.sum(hidden.astype(jnp.float32) * hid_grad, axis=1)
    down_grad = jnp.dot(hidden.T, cotan, preferred_element_type=jnp.float32).astype(jnp.bfloat16)
    gate_grad = jnp.dot(rows.T, gate_part, preferred_element_type=jnp.float32).astype(jnp.bfloat16)
    up_grad = jnp.dot(rows.T, up_part, preferred_element_type=jnp.float32).astype(jnp.bfloat16)
    return gate_part, up_part, slot_dots, gate_grad, up_grad, down_grad


def reference(tokens, out_grad, routes, gates, gate_weight, up_weight, down_weight):
    slot_count = TOKENS * TOPK
    flat = jnp.arange(slot_count, dtype=jnp.int32)
    token_of = (flat // TOPK).astype(jnp.int32)
    flat_expert = routes.reshape(-1).astype(jnp.int32)
    onehot = (flat_expert[:, None] == jnp.arange(EXPERTS, dtype=jnp.int32)[None, :]).astype(jnp.int32)
    blocks = onehot.reshape(N_EP, TOK_DEV * TOPK, EXPERTS)
    before = jnp.cumsum(blocks, axis=1) - blocks
    slot_rank = jnp.sum(before * blocks, axis=2).reshape(-1)
    source = (flat // (TOK_DEV * TOPK)).astype(jnp.int32)
    slot_dest = (flat_expert * (N_EP * CAP) + source * CAP + slot_rank).astype(jnp.int32)
    owner = jnp.full((EXPERTS * N_EP * CAP,), slot_count, jnp.int32).at[slot_dest].set(flat)
    owner = owner.reshape(EXPERTS, N_EP * CAP)
    zero_row = jnp.zeros((1, D), jnp.bfloat16)
    row_table = jnp.concatenate([tokens[token_of], zero_row], axis=0)
    scaled = (gates.reshape(-1)[:, None] * out_grad[token_of].astype(jnp.float32)).astype(jnp.bfloat16)
    cotan_table = jnp.concatenate([scaled, zero_row], axis=0)
    width = FF // N_TP

    def per_expert(inputs):
        index, w_gate, w_up, w_down = inputs
        rows = row_table[index]
        cotan = cotan_table[index]
        gate_part, up_part, slot_dots, gate_grad, up_grad, down_grad = expert_grads(rows, cotan, w_gate, w_up, w_down)
        count = index.shape[0]
        parts_gate = gate_part.reshape(count, N_TP, width).transpose(1, 0, 2)
        parts_up = up_part.reshape(count, N_TP, width).transpose(1, 0, 2)
        split_gate = w_gate.reshape(D, N_TP, width).transpose(1, 0, 2)
        split_up = w_up.reshape(D, N_TP, width).transpose(1, 0, 2)

        def add_slice(total, pieces):
            piece_gate, piece_up, weight_gate, weight_up = pieces
            term = jnp.dot(piece_gate, weight_gate.T, preferred_element_type=jnp.float32)
            term = term + jnp.dot(piece_up, weight_up.T, preferred_element_type=jnp.float32)
            rounded = lax.optimization_barrier(term.astype(jnp.bfloat16))
            return total + rounded.astype(jnp.float32), None

        row_grad, _ = lax.scan(add_slice, jnp.zeros((count, D), jnp.float32),
                               (parts_gate, parts_up, split_gate, split_up))
        return gate_grad, up_grad, down_grad, row_grad, slot_dots

    gate_grads, up_grads, down_grads, row_grads, dots = lax.map(
        per_expert, (owner, gate_weight, up_weight, down_weight))
    targets = owner.reshape(-1)
    slot_grad = jnp.zeros((slot_count + 1, D), jnp.float32).at[targets].add(row_grads.reshape(-1, D))
    tokens_grad = jnp.sum(slot_grad[:slot_count].reshape(TOKENS, TOPK, D), axis=1).astype(jnp.bfloat16)
    slot_dot = jnp.zeros((slot_count + 1,), jnp.float32).at[targets].add(dots.reshape(-1))
    gates_grad = slot_dot[:slot_count].reshape(TOKENS, TOPK) / gates
    return tokens_grad, gates_grad, gate_grads, up_grads, down_grads
```

```python
import jax
import jax.numpy as jnp
from jax import lax
from jax.sharding import Mesh
from jax.sharding import PartitionSpec as P

TP = ("y", "x")
BF16 = jnp.bfloat16
F32 = jnp.float32


def exchange(array, axis):
    return lax.all_to_all(array, axis, split_axis=0, concat_axis=0, tiled=True)


def to_all(array, axis):
    copies = jnp.broadcast_to(array[None], (lax.axis_size(axis), *array.shape))
    return exchange(copies, axis)


def two_rows(values):
    high = values.astype(BF16)
    low = (values - high.astype(F32)).astype(BF16)
    return jnp.concatenate([high[..., None, :], low[..., None, :]], axis=-2)


def add_up(parts):
    total = jnp.sum(parts.astype(F32), axis=0)
    dots = total[..., -8, :] + total[..., -7, :]
    return total[..., :-8, :], dots


def with_dots(rows, dots):
    pad = [(0, 0)] * (rows.ndim - 2) + [(0, 6), (0, 0)]
    return jnp.concatenate([rows.astype(BF16), jnp.pad(two_rows(dots), pad)], axis=-2)


def on_device(tokens, out_grad, routes, gates, gate_weight, up_weight, down_weight):
    tok_dev, top_k = routes.shape
    n_ep, n_y, n_x = lax.axis_size("ep"), lax.axis_size("y"), lax.axis_size("x")
    cap = (3 * tok_dev + n_ep - 1) // n_ep
    rows = n_ep * cap
    feats = tokens.shape[1]
    width = n_y * n_x * feats
    flat = routes.T.reshape(-1)
    slots = flat.shape[0]
    before = jnp.arange(slots)[None, :] < jnp.arange(slots)[:, None]
    same = (flat[None, :] == flat[:, None]) & before
    dest = (flat * cap + jnp.sum(same.astype(jnp.int32), axis=1)).reshape(top_k, tok_dev)
    place = jnp.arange(rows, dtype=jnp.int32)[:, None]
    at = [place == dest[k][None, :] for k in range(top_k)]
    select = (at[0] | at[1]).astype(BF16)
    slot_gate = sum(jnp.sum(jnp.where(at[k], gates[:, k][None, :], 0.0), axis=1) for k in range(top_k))
    both = jnp.dot(select, jnp.concatenate([tokens, out_grad], axis=1), preferred_element_type=F32)
    scale = jnp.where(jnp.arange(2 * feats)[None, :] < feats, 1.0, slot_gate[:, None])
    sent = (both * scale).astype(BF16)

    got = exchange(sent.reshape(n_ep, cap, 2 * feats), "ep").reshape(rows, 2 * feats)
    by_y = to_all(got.T, "y")
    by_xy = to_all(by_y, "x").reshape(n_x, n_y, 2, feats, rows)
    x_t = by_xy[:, :, 0].transpose(1, 0, 2, 3).reshape(width, rows)
    c_t = by_xy[:, :, 1].transpose(1, 0, 2, 3).reshape(width, rows)

    w_gate, w_up, w_down = gate_weight[0].T, up_weight[0].T, down_weight[0]
    pre_gate = jnp.dot(w_gate, x_t, preferred_element_type=F32)
    pre_up = jnp.dot(w_up, x_t, preferred_element_type=F32)
    hid_grad = jnp.dot(w_down, c_t, preferred_element_type=F32)
    sig = jax.nn.sigmoid(pre_gate)
    act = pre_gate * sig
    hidden = (act * pre_up).astype(BF16)
    gate_part = (hid_grad * pre_up * sig * (1.0 + pre_gate * (1.0 - sig))).astype(BF16)
    up_part = (hid_grad * act).astype(BF16)
    dots = jnp.sum(hidden.astype(F32) * hid_grad, axis=0)

    def dot_t(a, b, dims):
        return lax.dot_general(a, b, (dims, ((), ())), preferred_element_type=F32)

    piece = dot_t(w_gate, gate_part, ((0,), (0,))) + dot_t(w_up, up_part, ((0,), (0,)))
    piece = piece.astype(BF16).reshape(n_y, n_x, feats, rows).transpose(1, 0, 2, 3)
    chunks = with_dots(piece, jnp.broadcast_to(dots, (n_x, n_y, rows)))
    near, near_dots = add_up(exchange(chunks, "x"))

    gate_grad = dot_t(gate_part, x_t, ((1,), (1,))).astype(BF16)
    up_grad = dot_t(up_part, x_t, ((1,), (1,))).astype(BF16)
    down_grad = dot_t(hidden, c_t, ((1,), (1,))).astype(BF16)

    row_sum, all_dots = add_up(exchange(with_dots(near, near_dots), "y"))
    packed = jnp.concatenate([row_sum.astype(BF16), two_rows(all_dots)], axis=0)
    packed = jnp.pad(packed, ((0, 2 * feats - packed.shape[0]), (0, 0))).T
    back = exchange(packed.reshape(n_ep, cap, 2 * feats), "ep").reshape(rows, 2 * feats)
    tokens_grad = dot_t(select, back, ((0,), (0,)))[:, :feats].astype(BF16)
    share = tok_dev // (n_y * n_x)
    start = lax.axis_index(TP) * share
    own_dest = lax.dynamic_slice_in_dim(dest, start, share, 1).T
    own_gates = lax.dynamic_slice_in_dim(gates, start, share, 0)
    back_dots = back[:, feats].astype(F32) + back[:, feats + 1].astype(F32)
    mine = own_dest[:, :, None] == jnp.arange(rows, dtype=jnp.int32)
    own_dots = jnp.sum(jnp.where(mine, back_dots, 0.0), axis=2)
    return (
        tokens_grad,
        own_dots / own_gates,
        gate_grad.T[None],
        up_grad.T[None],
        down_grad[None],
    )


def solution(mesh):
    torus = Mesh(mesh.devices.reshape(mesh.shape["ep"], 8, 4), ("ep", "y", "x"))
    return jax.shard_map(
        on_device,
        mesh=torus,
        in_specs=(
            P("ep", TP),
            P("ep", TP),
            P("ep", None),
            P("ep", None),
            P("ep", None, TP),
            P("ep", None, TP),
            P("ep", TP, None),
        ),
        out_specs=(
            P("ep", TP),
            P(("ep", "y", "x"), None),
            P("ep", None, TP),
            P("ep", None, TP),
            P("ep", TP, None),
        ),
        check_vma=False,
    )
```

```python
import functools

import jax
import jax.numpy as jnp
from jax import lax
from jax.experimental import pallas as pl
from jax.experimental.pallas import tpu as pltpu
from jax.sharding import Mesh
from jax.sharding import PartitionSpec as P

TP = ("y", "x")
BF16 = jnp.bfloat16
F32 = jnp.float32
I32 = jnp.int32
CPU_INTERPRET = False


def call(body, outs, flops=0, n_scalars=0, scratch=(), away=(), out_away=(), limit=12):
    def run(*args):
        smem = pl.BlockSpec(memory_space=pltpu.SMEM)
        vmem = pl.BlockSpec(memory_space=pltpu.VMEM)
        anywhere = pl.BlockSpec(memory_space=pltpu.HBM)
        size = sum(a.size * a.dtype.itemsize for a in args)
        return pl.pallas_call(
            body,
            out_shape=[jax.ShapeDtypeStruct(s, d) for s, d in outs],
            in_specs=[
                smem if k < n_scalars else anywhere if k in away else vmem
                for k in range(len(args))
            ],
            out_specs=[anywhere if k in out_away else vmem for k in range(len(outs))],
            scratch_shapes=list(scratch),
            compiler_params=pltpu.CompilerParams(vmem_limit_bytes=limit * 2**20),
            cost_estimate=pl.CostEstimate(flops=flops, transcendentals=0, bytes_accessed=size),
            interpret=CPU_INTERPRET,
        )(*args)

    return run


def dot(a, b, dims):
    return lax.dot_general(a, b, (dims, ((), ())), preferred_element_type=F32)


def iota(shape, dim):
    return lax.broadcasted_iota(I32, shape, dim)


def dot_rows(dots):
    high = dots.astype(BF16).astype(F32)
    row = iota((8, dots.shape[1]), 0)
    return jnp.where(row == 0, high, jnp.where(row == 1, dots - high, 0.0))


def place_body(routes_ref, gates_ref, tokens_ref, grad_ref, sent_ref, dest_ref, *, n_ep, cap):
    routes = routes_ref[...]
    top_k, toks = routes.shape
    experts = -(-n_ep // 16) * 16
    hot = [(iota((experts, toks), 0) == routes[k : k + 1]).astype(BF16) for k in range(top_k)]
    hot = jnp.concatenate(hot, axis=1)
    slots = top_k * toks
    earlier = (iota((slots, slots), 0) < iota((slots, slots), 1)).astype(BF16)
    rank = jnp.sum(dot(hot, earlier, ((1,), (0,))) * hot.astype(F32), axis=0, keepdims=True)
    rank = rank.astype(I32)
    rows = n_ep * cap
    place = iota((rows, toks), 0)
    select = jnp.zeros((rows, toks), F32)
    weight = jnp.zeros((rows, 1), F32)
    for k in range(top_k):
        dest = routes[k : k + 1] * cap + rank[:, k * toks : (k + 1) * toks]
        dest_ref[k : k + 1, :] = dest
        at = place == dest
        select = select + jnp.where(at, 1.0, 0.0)
        weight = weight + jnp.sum(jnp.where(at, gates_ref[k : k + 1, :], 0.0), axis=1, keepdims=True)
    both = jnp.concatenate([tokens_ref[...], grad_ref[...]], axis=0)
    feats = tokens_ref.shape[0]
    moved = dot(select.astype(BF16), both, ((1,), (1,)))
    lane = iota(moved.shape, 1)
    sent_ref[...] = jnp.where(lane < feats, moved, moved * weight).astype(BF16)


def turn_body(got_ref, out_ref):
    turned = got_ref[...].astype(F32).T.astype(BF16)
    for k in range(out_ref.shape[0]):
        out_ref[k] = turned


def expert_body(
    order_ref, own_ref, left_ref, right_ref, far_a_ref, far_b_ref, wg_any, wu_any, wd_any,
    out_ref, parts_ref, x_out, c_out,
    wg_ref, wu_ref, wd_ref, far_ref, x_ref, c_ref, sems,
):
    n_y, both, rows = own_ref.shape
    feats = both // 2
    hid = wg_ref.shape[0]
    n_x = out_ref.shape[0]
    half = far_a_ref.shape[0]
    fetches = [
        pltpu.make_async_copy(src, dst, sems.at[k])
        for k, (src, dst) in enumerate(
            (
                (far_a_ref, far_ref.at[pl.ds(0, half)]),
                (far_b_ref, far_ref.at[pl.ds(half, n_y - half)]),
                (wg_any, wg_ref),
                (wu_any, wu_ref),
                (wd_any, wd_ref),
            )
        )
    ]
    for fetch in fetches:
        fetch.start()
    for k, source in enumerate((own_ref, left_ref, right_ref, far_ref)):
        if k == 3:
            fetches[0].wait()
            fetches[1].wait()
        at = order_ref[k]
        for y in range(n_y):
            x_ref[y, at] = source[y, :feats]
            c_ref[y, at] = source[y, feats:]
    saves = [
        pltpu.make_async_copy(x_ref, x_out, sems.at[5]),
        pltpu.make_async_copy(c_ref, c_out, sems.at[6]),
    ]
    for save in saves:
        save.start()
    width = n_y * n_x * feats
    x_t = x_ref[...].reshape(width, rows)
    c_t = c_ref[...].reshape(width, rows)
    fetches[2].wait()
    pre_gate = jnp.dot(wg_ref[...], x_t, preferred_element_type=F32)
    fetches[3].wait()
    pre_up = jnp.dot(wu_ref[...], x_t, preferred_element_type=F32)
    fetches[4].wait()
    hid_grad = jnp.dot(wd_ref[...], c_t, preferred_element_type=F32)
    sig = jax.nn.sigmoid(pre_gate)
    act = pre_gate * sig
    hidden = (act * pre_up).astype(BF16)
    gate_part = (hid_grad * pre_up * sig * (1.0 + pre_gate * (1.0 - sig))).astype(BF16)
    up_part = (hid_grad * act).astype(BF16)
    dots = jnp.sum(hidden.astype(F32) * hid_grad, axis=0, keepdims=True)
    parts_ref[0:hid] = gate_part
    parts_ref[hid : 2 * hid] = up_part
    parts_ref[2 * hid : 3 * hid] = hidden
    parts = parts_ref[0 : 2 * hid]
    tail = dot_rows(dots).astype(BF16)
    for y in range(n_y):
        cols = slice(y * n_x * feats, (y + 1) * n_x * feats)
        w = jnp.concatenate([wg_ref[:, cols], wu_ref[:, cols]], axis=0)
        piece = dot(w, parts, ((0,), (0,))).astype(BF16)
        for x in range(n_x):
            out_ref[x, y * feats : (y + 1) * feats] = piece[x * feats : (x + 1) * feats]
    for x in range(n_x):
        out_ref[x, n_y * feats :] = tail
    for save in saves:
        save.wait()


def weights_body(parts_ref, x_ref, c_ref, gate_ref, up_ref, down_ref):
    n_y, n_x, feats, rows = x_ref.shape
    hid = gate_ref.shape[0]
    for y in range(n_y):
        cols = slice(y * n_x * feats, (y + 1) * n_x * feats)
        x_t = x_ref[y].reshape(n_x * feats, rows)
        c_t = c_ref[y].reshape(n_x * feats, rows)
        grads = dot(parts_ref[0 : 2 * hid], x_t, ((1,), (1,))).astype(BF16)
        gate_ref[:, cols] = grads[:hid]
        up_ref[:, cols] = grads[hid:]
        down_ref[:, cols] = dot(parts_ref[2 * hid :], c_t, ((1,), (1,))).astype(BF16)


def near_body(in_ref, out_ref):
    n, height, _ = in_ref.shape
    n_y, tall, _ = out_ref.shape
    feats = tall - 8
    for y in range(n_y):
        total = in_ref[0, y * feats : (y + 1) * feats].astype(F32)
        for k in range(1, n):
            total = total + in_ref[k, y * feats : (y + 1) * feats].astype(F32)
        out_ref[y, :feats] = total.astype(BF16)
    tail = in_ref[0, height - 8 :].astype(F32)
    for k in range(1, n):
        tail = tail + in_ref[k, height - 8 :].astype(F32)
    tail = dot_rows(jnp.sum(tail, axis=0, keepdims=True)).astype(BF16)
    for y in range(n_y):
        out_ref[y, feats:] = tail


def far_body(in_ref, out_ref):
    n, tall, rows = in_ref.shape
    total = in_ref[0].astype(F32)
    for k in range(1, n):
        total = total + in_ref[k].astype(F32)
    feats = tall - 8
    tail = dot_rows(jnp.sum(total[feats:], axis=0, keepdims=True))
    rest = jnp.zeros((out_ref.shape[1] - tall, rows), F32)
    whole = jnp.concatenate([total[:feats], tail, rest], axis=0)
    out_ref[...] = whole.T.astype(BF16)


def final_body(start_ref, back_ref, dest_ref, gates_ref, tokens_ref, ratio_ref):
    rows, lanes = back_ref.shape
    feats, toks = tokens_ref.shape
    top_k, share = ratio_ref.shape
    back = back_ref[...]
    dots = back[:, feats : feats + 1].astype(F32) + back[:, feats + 1 : feats + 2].astype(F32)
    place = iota((rows, toks), 0)
    select = jnp.zeros((rows, toks), F32)
    start = start_ref[0]
    for k in range(top_k):
        at = place == dest_ref[k : k + 1, :]
        select = select + jnp.where(at, 1.0, 0.0)
        mine = jnp.sum(jnp.where(at, dots, 0.0), axis=0, keepdims=True) / gates_ref[k : k + 1, :]
        for j in range(share):
            here = iota((1, toks), 1) == start + j
            ratio_ref[k : k + 1, j : j + 1] = jnp.sum(jnp.where(here, mine, 0.0), axis=1, keepdims=True)
    summed = dot(back, select.astype(BF16), ((0,), (0,)))
    tokens_ref[...] = summed[:feats].astype(BF16)


def exchange(array, axis):
    return lax.all_to_all(array, axis, split_axis=0, concat_axis=0, tiled=True)


def shift(array, axis, by):
    n = lax.axis_size(axis)
    return lax.ppermute(array, axis, [(k, (k + by) % n) for k in range(n)])


def on_device(tokens, out_grad, routes, gates, gate_weight, up_weight, down_weight):
    tok_dev, top_k = routes.shape
    n_ep, n_y, n_x = lax.axis_size("ep"), lax.axis_size("y"), lax.axis_size("x")
    cap = (3 * tok_dev + n_ep - 1) // n_ep
    rows = n_ep * cap
    feats = tokens.shape[1]
    both = 2 * feats
    w_gate, w_up, w_down = gate_weight[0].T, up_weight[0].T, down_weight[0]
    hid, width = w_gate.shape

    sent, dest = call(
        functools.partial(place_body, n_ep=n_ep, cap=cap),
        [((rows, both), BF16), ((top_k, tok_dev), I32)],
    )(routes.T, gates.T, tokens.T, out_grad.T)
    got = exchange(sent.reshape(n_ep, cap, both), "ep").reshape(rows, both)
    (copies,) = call(turn_body, [((n_y, both, rows), BF16)])(got)
    own = exchange(copies, "y")
    left, right = shift(own, "x", 1), shift(own, "x", -1)
    half = n_y // 2
    far_a, far_b = shift(left[:half], "x", 1), shift(right[half:], "x", -1)

    my_x = lax.axis_index("x").astype(I32)
    order = (my_x + jnp.array([0, n_x - 1, 1, 2], I32)) % n_x
    chunks, parts, x_t, c_t = call(
        expert_body,
        [
            ((n_x, n_y * feats + 8, rows), BF16),
            ((3 * hid, rows), BF16),
            ((n_y, n_x, feats, rows), BF16),
            ((n_y, n_x, feats, rows), BF16),
        ],
        flops=10 * hid * width * rows,
        n_scalars=1,
        away=(4, 5, 6, 7, 8),
        out_away=(2, 3),
        limit=24,
        scratch=[pltpu.VMEM((hid, width), BF16)] * 3
        + [pltpu.VMEM((n_y, both, rows), BF16)]
        + [pltpu.VMEM((n_y, n_x, feats, rows), BF16)] * 2
        + [pltpu.SemaphoreType.DMA((7,))],
    )(order, own, left, right, far_a, far_b, w_gate, w_up, w_down)
    swapped = exchange(chunks, "x")
    gate_grad, up_grad, down_grad = call(
        weights_body, [((hid, width), BF16)] * 3, flops=6 * hid * width * rows, limit=24
    )(parts, x_t, c_t)
    (near,) = call(near_body, [((n_y, feats + 8, rows), BF16)])(swapped)
    (packed,) = call(far_body, [((rows, both), BF16)])(exchange(near, "y"))
    back = exchange(packed.reshape(n_ep, cap, both), "ep").reshape(rows, both)
    share = tok_dev // (n_y * n_x)
    start = (lax.axis_index(TP).astype(I32) * share).reshape(1)
    tokens_grad, ratio = call(
        final_body, [((feats, tok_dev), BF16), ((top_k, share), F32)], n_scalars=1
    )(start, back, dest, gates.T)
    return (
        tokens_grad.T,
        ratio.T,
        gate_grad.T[None],
        up_grad.T[None],
        down_grad[None],
    )


def solution(mesh):
    torus = Mesh(mesh.devices.reshape(mesh.shape["ep"], 8, 4), ("ep", "y", "x"))
    return jax.shard_map(
        on_device,
        mesh=torus,
        in_specs=(
            P("ep", TP),
            P("ep", TP),
            P("ep", None),
            P("ep", None),
            P("ep", None, TP),
            P("ep", None, TP),
            P("ep", TP, None),
        ),
        out_specs=(
            P("ep", TP),
            P(("ep", "y", "x"), None),
            P("ep", None, TP),
            P("ep", None, TP),
            P("ep", TP, None),
        ),
        check_vma=False,
    )
```

```python
import functools

import jax
import jax.numpy as jnp
from jax import lax
from jax.experimental import pallas as pl
from jax.experimental.pallas import tpu as pltpu
from jax.sharding import Mesh
from jax.sharding import PartitionSpec as P

TP = ("yh", "yl", "x")
NEAR = ("yl", "x")
BF16 = jnp.bfloat16
F32 = jnp.float32
I32 = jnp.int32
CPU_INTERPRET = False


def call(body, outs, flops=0, n_scalars=0, limit=12):
    def run(*args):
        smem = pl.BlockSpec(memory_space=pltpu.SMEM)
        vmem = pl.BlockSpec(memory_space=pltpu.VMEM)
        size = sum(a.size * a.dtype.itemsize for a in args)
        return pl.pallas_call(
            body,
            out_shape=[jax.ShapeDtypeStruct(s, d) for s, d in outs],
            in_specs=[smem if k < n_scalars else vmem for k in range(len(args))],
            out_specs=[vmem] * len(outs),
            compiler_params=pltpu.CompilerParams(vmem_limit_bytes=limit * 2**20),
            cost_estimate=pl.CostEstimate(flops=flops, transcendentals=0, bytes_accessed=size),
            interpret=CPU_INTERPRET,
        )(*args)

    return run


def dot(a, b, dims):
    return lax.dot_general(a, b, (dims, ((), ())), preferred_element_type=F32)


def iota(shape, dim):
    return lax.broadcasted_iota(I32, shape, dim)


def dot_rows(dots):
    high = dots.astype(BF16).astype(F32)
    row = iota((8, dots.shape[1]), 0)
    return jnp.where(row == 0, high, jnp.where(row == 1, dots - high, 0.0))


def place_body(table_ref, sent_ref, dest_ref, *, n_ep, cap, top_k):
    toks = table_ref.shape[1]
    both = table_ref.shape[0] - 2 * top_k
    feats = both // 2
    routes = table_ref[both : both + top_k].astype(I32)
    gates = table_ref[both + top_k :]
    experts = -(-n_ep // 16) * 16
    hot = [(iota((experts, toks), 0) == routes[k : k + 1]).astype(BF16) for k in range(top_k)]
    hot = jnp.concatenate(hot, axis=1)
    slots = top_k * toks
    earlier = (iota((slots, slots), 0) < iota((slots, slots), 1)).astype(BF16)
    rank = jnp.sum(dot(hot, earlier, ((1,), (0,))) * hot.astype(F32), axis=0, keepdims=True)
    rank = rank.astype(I32)
    rows = n_ep * cap
    place = iota((rows, toks), 0)
    select = jnp.zeros((rows, toks), F32)
    weight = jnp.zeros((rows, 1), F32)
    for k in range(top_k):
        dest = routes[k : k + 1] * cap + rank[:, k * toks : (k + 1) * toks]
        dest_ref[k : k + 1, :] = dest
        at = place == dest
        select = select + jnp.where(at, 1.0, 0.0)
        weight = weight + jnp.sum(jnp.where(at, gates[k : k + 1], 0.0), axis=1, keepdims=True)
    moved = dot(select.astype(BF16), table_ref[:both].astype(BF16), ((1,), (1,)))
    lane = iota(moved.shape, 1)
    sent_ref[...] = jnp.where(lane < feats, moved, moved * weight).astype(BF16)


def turn_body(got_ref, out_ref):
    turned = got_ref[...].astype(F32).T.astype(BF16)
    for k in range(out_ref.shape[0]):
        out_ref[k] = turned


def column(rows_ref, yh, yl, part):
    _, _, both, _ = rows_ref.shape
    feats = both // 2
    n_x = rows_ref.shape[0] // 2
    at = slice(part * feats, (part + 1) * feats)
    return jnp.concatenate([rows_ref[yl * n_x + x, yh, at] for x in range(n_x)], axis=0)


def expert_body(rows_ref, wg_ref, wu_ref, wd_ref, out_ref, parts_ref):
    n_near, n_yh, both, _ = rows_ref.shape
    feats = both // 2
    n_x = n_near // 2
    hid = wg_ref.shape[0]
    order = [(yh, yl) for yh in range(n_yh) for yl in range(2)]
    x_t = jnp.concatenate([column(rows_ref, yh, yl, 0) for yh, yl in order], axis=0)
    pre_gate = jnp.dot(wg_ref[...], x_t, preferred_element_type=F32)
    pre_up = jnp.dot(wu_ref[...], x_t, preferred_element_type=F32)
    c_t = jnp.concatenate([column(rows_ref, yh, yl, 1) for yh, yl in order], axis=0)
    hid_grad = jnp.dot(wd_ref[...], c_t, preferred_element_type=F32)
    sig = jax.nn.sigmoid(pre_gate)
    act = pre_gate * sig
    hidden = (act * pre_up).astype(BF16)
    gate_part = (hid_grad * pre_up * sig * (1.0 + pre_gate * (1.0 - sig))).astype(BF16)
    up_part = (hid_grad * act).astype(BF16)
    dots = jnp.sum(hidden.astype(F32) * hid_grad, axis=0, keepdims=True)
    parts_ref[0:hid] = gate_part
    parts_ref[hid : 2 * hid] = up_part
    parts_ref[2 * hid : 3 * hid] = hidden
    parts = parts_ref[0 : 2 * hid]
    tail = dot_rows(dots).astype(BF16)
    for k, (yh, yl) in enumerate(order):
        cols = slice(k * n_x * feats, (k + 1) * n_x * feats)
        w = jnp.concatenate([wg_ref[:, cols], wu_ref[:, cols]], axis=0)
        piece = dot(w, parts, ((0,), (0,))).astype(BF16)
        for x in range(n_x):
            at = slice(yh * feats, (yh + 1) * feats)
            out_ref[yl * n_x + x, at] = piece[x * feats : (x + 1) * feats]
    for k in range(n_near):
        out_ref[k, n_yh * feats :] = tail


def weights_body(parts_ref, rows_ref, gate_ref, up_ref, down_ref):
    n_near, n_yh, both, _ = rows_ref.shape
    wide = n_near // 2 * (both // 2)
    hid = gate_ref.shape[0]
    for yh in range(n_yh):
        for yl in range(2):
            k = 2 * yh + yl
            cols = slice(k * wide, (k + 1) * wide)
            x_t, c_t = column(rows_ref, yh, yl, 0), column(rows_ref, yh, yl, 1)
            grads = dot(parts_ref[0 : 2 * hid], x_t, ((1,), (1,))).astype(BF16)
            gate_ref[:, cols] = grads[:hid]
            up_ref[:, cols] = grads[hid:]
            down_ref[:, cols] = dot(parts_ref[2 * hid :], c_t, ((1,), (1,))).astype(BF16)


def near_body(in_ref, out_ref):
    n, height, _ = in_ref.shape
    n_y, tall, _ = out_ref.shape
    feats = tall - 8
    for y in range(n_y):
        total = in_ref[0, y * feats : (y + 1) * feats].astype(F32)
        for k in range(1, n):
            total = total + in_ref[k, y * feats : (y + 1) * feats].astype(F32)
        out_ref[y, :feats] = total.astype(BF16)
    tail = in_ref[0, height - 8 :].astype(F32)
    for k in range(1, n):
        tail = tail + in_ref[k, height - 8 :].astype(F32)
    tail = dot_rows(jnp.sum(tail, axis=0, keepdims=True)).astype(BF16)
    for y in range(n_y):
        out_ref[y, feats:] = tail


def far_body(in_ref, out_ref):
    n, tall, rows = in_ref.shape
    total = in_ref[0].astype(F32)
    for k in range(1, n):
        total = total + in_ref[k].astype(F32)
    feats = tall - 8
    tail = dot_rows(jnp.sum(total[feats:], axis=0, keepdims=True))
    rest = jnp.zeros((out_ref.shape[1] - tall, rows), F32)
    whole = jnp.concatenate([total[:feats], tail, rest], axis=0)
    out_ref[...] = whole.T.astype(BF16)


def final_body(start_ref, back_ref, dest_ref, gates_ref, tokens_ref, ratio_ref):
    rows, lanes = back_ref.shape
    feats, toks = tokens_ref.shape
    top_k, share = ratio_ref.shape
    back = back_ref[...]
    dots = back[:, feats : feats + 1].astype(F32) + back[:, feats + 1 : feats + 2].astype(F32)
    place = iota((rows, toks), 0)
    select = jnp.zeros((rows, toks), F32)
    start = start_ref[0]
    for k in range(top_k):
        at = place == dest_ref[k : k + 1, :]
        select = select + jnp.where(at, 1.0, 0.0)
        mine = jnp.sum(jnp.where(at, dots, 0.0), axis=0, keepdims=True) / gates_ref[k : k + 1, :]
        for j in range(share):
            here = iota((1, toks), 1) == start + j
            ratio_ref[k : k + 1, j : j + 1] = jnp.sum(jnp.where(here, mine, 0.0), axis=1, keepdims=True)
    summed = dot(back, select.astype(BF16), ((0,), (0,)))
    tokens_ref[...] = summed[:feats].astype(BF16)


def exchange(array, axis):
    return lax.all_to_all(array, axis, split_axis=0, concat_axis=0, tiled=True)


def on_device(tokens, out_grad, routes, gates, gate_weight, up_weight, down_weight):
    tok_dev, top_k = routes.shape
    n_ep, n_yh, n_near = lax.axis_size("ep"), lax.axis_size("yh"), lax.axis_size(NEAR)
    cap = (3 * tok_dev + n_ep - 1) // n_ep
    rows = n_ep * cap
    feats = tokens.shape[1]
    both = 2 * feats
    w_gate, w_up, w_down = gate_weight[0].T, up_weight[0].T, down_weight[0]
    hid, width = w_gate.shape

    table = jnp.concatenate(
        [a.T.astype(F32) for a in (tokens, out_grad, routes, gates)], axis=0
    )
    sent, dest = call(
        functools.partial(place_body, n_ep=n_ep, cap=cap, top_k=top_k),
        [((rows, both), BF16), ((top_k, tok_dev), I32)],
    )(table)
    got = exchange(sent.reshape(n_ep, cap, both), "ep").reshape(rows, both)
    (copies,) = call(turn_body, [((n_yh, both, rows), BF16)])(got)
    some = exchange(copies, "yh")
    every = exchange(jnp.broadcast_to(some[None], (n_near, *some.shape)), NEAR)

    chunks, parts = call(
        expert_body,
        [((n_near, n_yh * feats + 8, rows), BF16), ((3 * hid, rows), BF16)],
        flops=10 * hid * width * rows,
        limit=20,
    )(every, w_gate, w_up, w_down)
    swapped = exchange(chunks, NEAR)
    gate_grad, up_grad, down_grad = call(
        weights_body, [((hid, width), BF16)] * 3, flops=6 * hid * width * rows, limit=20
    )(parts, every)
    (near,) = call(near_body, [((n_yh, feats + 8, rows), BF16)])(swapped)
    (packed,) = call(far_body, [((rows, both), BF16)])(exchange(near, "yh"))
    back = exchange(packed.reshape(n_ep, cap, both), "ep").reshape(rows, both)
    share = tok_dev // (n_yh * n_near)
    start = (lax.axis_index(TP).astype(I32) * share).reshape(1)
    tokens_grad, ratio = call(
        final_body, [((feats, tok_dev), BF16), ((top_k, share), F32)], n_scalars=1
    )(start, back, dest, gates.T)
    return (
        tokens_grad.T,
        ratio.T,
        gate_grad.T[None],
        up_grad.T[None],
        down_grad[None],
    )


def solution(mesh):
    torus = Mesh(mesh.devices.reshape(mesh.shape["ep"], 4, 2, 4), ("ep", *TP))
    return jax.shard_map(
        on_device,
        mesh=torus,
        in_specs=(
            P("ep", TP),
            P("ep", TP),
            P("ep", None),
            P("ep", None),
            P("ep", None, TP),
            P("ep", None, TP),
            P("ep", TP, None),
        ),
        out_specs=(
            P("ep", TP),
            P(("ep", *TP), None),
            P("ep", None, TP),
            P("ep", None, TP),
            P("ep", TP, None),
        ),
        check_vma=False,
    )
```

```python
import functools

import jax
import jax.numpy as jnp
from jax import lax
from jax.experimental import pallas as pl
from jax.experimental.pallas import tpu as pltpu
from jax.sharding import Mesh
from jax.sharding import PartitionSpec as P

TP = ("yh", "yl", "x")
NEAR = ("yl", "x")
BF16 = jnp.bfloat16
F32 = jnp.float32
I32 = jnp.int32
CPU_INTERPRET = False


def call(body, outs, flops=0, n_scalars=0, limit=12):
    def run(*args):
        smem = pl.BlockSpec(memory_space=pltpu.SMEM)
        vmem = pl.BlockSpec(memory_space=pltpu.VMEM)
        size = sum(a.size * a.dtype.itemsize for a in args)
        return pl.pallas_call(
            body,
            out_shape=[jax.ShapeDtypeStruct(s, d) for s, d in outs],
            in_specs=[smem if k < n_scalars else vmem for k in range(len(args))],
            out_specs=[vmem] * len(outs),
            compiler_params=pltpu.CompilerParams(vmem_limit_bytes=limit * 2**20),
            cost_estimate=pl.CostEstimate(flops=flops, transcendentals=0, bytes_accessed=size),
            interpret=CPU_INTERPRET,
        )(*args)

    return run


def dot(a, b, dims):
    return lax.dot_general(a, b, (dims, ((), ())), preferred_element_type=F32)


def iota(shape, dim):
    return lax.broadcasted_iota(I32, shape, dim)


def dot_rows(dots):
    high = dots.astype(BF16).astype(F32)
    row = iota((8, dots.shape[1]), 0)
    return jnp.where(row == 0, high, jnp.where(row == 1, dots - high, 0.0))


def place_body(table_ref, sent_ref, dest_ref, *, n_ep, cap, top_k):
    toks = table_ref.shape[1]
    both = table_ref.shape[0] - 2 * top_k
    feats = both // 2
    routes = table_ref[both : both + top_k].astype(I32)
    gates = table_ref[both + top_k :]
    experts = -(-n_ep // 16) * 16
    hot = [(iota((experts, toks), 0) == routes[k : k + 1]).astype(BF16) for k in range(top_k)]
    hot = jnp.concatenate(hot, axis=1)
    slots = top_k * toks
    earlier = (iota((slots, slots), 0) < iota((slots, slots), 1)).astype(BF16)
    rank = jnp.sum(dot(hot, earlier, ((1,), (0,))) * hot.astype(F32), axis=0, keepdims=True)
    rank = rank.astype(I32)
    rows = n_ep * cap
    place = iota((rows, toks), 0)
    select = jnp.zeros((rows, toks), F32)
    weight = jnp.zeros((rows, 1), F32)
    for k in range(top_k):
        dest = routes[k : k + 1] * cap + rank[:, k * toks : (k + 1) * toks]
        dest_ref[k : k + 1, :] = dest
        at = place == dest
        select = select + jnp.where(at, 1.0, 0.0)
        weight = weight + jnp.sum(jnp.where(at, gates[k : k + 1], 0.0), axis=1, keepdims=True)
    moved = dot(select.astype(BF16), table_ref[:both].astype(BF16), ((1,), (1,)))
    lane = iota(moved.shape, 1)
    sent_ref[...] = jnp.where(lane < feats, moved, moved * weight).astype(BF16)


def turn_body(got_ref, out_ref):
    turned = got_ref[...].astype(F32).T.astype(BF16)
    for k in range(out_ref.shape[0]):
        out_ref[k] = turned


def column(rows_ref, yh, yl, part):
    _, _, both, _ = rows_ref.shape
    feats = both // 2
    n_x = rows_ref.shape[0] // 2
    at = slice(part * feats, (part + 1) * feats)
    return jnp.concatenate([rows_ref[yl * n_x + x, yh, at] for x in range(n_x)], axis=0)


def expert_body(rows_ref, wg_ref, wu_ref, wd_ref, out_ref, parts_ref):
    n_near, n_yh, both, _ = rows_ref.shape
    feats = both // 2
    n_x = n_near // 2
    hid = wg_ref.shape[0]
    order = [(yh, yl) for yh in range(n_yh) for yl in range(2)]
    x_t = jnp.concatenate([column(rows_ref, yh, yl, 0) for yh, yl in order], axis=0)
    pre_gate = jnp.dot(wg_ref[...], x_t, preferred_element_type=F32)
    pre_up = jnp.dot(wu_ref[...], x_t, preferred_element_type=F32)
    c_t = jnp.concatenate([column(rows_ref, yh, yl, 1) for yh, yl in order], axis=0)
    hid_grad = jnp.dot(wd_ref[...], c_t, preferred_element_type=F32)
    sig = jax.nn.sigmoid(pre_gate)
    act = pre_gate * sig
    hidden = (act * pre_up).astype(BF16)
    gate_part = (hid_grad * pre_up * sig * (1.0 + pre_gate * (1.0 - sig))).astype(BF16)
    up_part = (hid_grad * act).astype(BF16)
    dots = jnp.sum(hidden.astype(F32) * hid_grad, axis=0, keepdims=True)
    parts_ref[0:hid] = gate_part
    parts_ref[hid : 2 * hid] = up_part
    parts_ref[2 * hid : 3 * hid] = hidden
    parts = parts_ref[0 : 2 * hid]
    tail = dot_rows(dots).astype(BF16)
    for k, (yh, yl) in enumerate(order):
        cols = slice(k * n_x * feats, (k + 1) * n_x * feats)
        w = jnp.concatenate([wg_ref[:, cols], wu_ref[:, cols]], axis=0)
        piece = dot(w, parts, ((0,), (0,))).astype(BF16)
        for x in range(n_x):
            at = slice(yh * feats, (yh + 1) * feats)
            out_ref[yl * n_x + x, at] = piece[x * feats : (x + 1) * feats]
    for k in range(n_near):
        out_ref[k, n_yh * feats :] = tail


def weights_body(parts_ref, rows_ref, gate_ref, up_ref, down_ref):
    n_near, n_yh, both, _ = rows_ref.shape
    wide = n_near // 2 * (both // 2)
    hid = gate_ref.shape[0]
    for yh in range(n_yh):
        for yl in range(2):
            k = 2 * yh + yl
            cols = slice(k * wide, (k + 1) * wide)
            x_t, c_t = column(rows_ref, yh, yl, 0), column(rows_ref, yh, yl, 1)
            grads = dot(parts_ref[0 : 2 * hid], x_t, ((1,), (1,))).astype(BF16)
            gate_ref[:, cols] = grads[:hid]
            up_ref[:, cols] = grads[hid:]
            down_ref[:, cols] = dot(parts_ref[2 * hid :], c_t, ((1,), (1,))).astype(BF16)


def near_body(in_ref, out_ref):
    n, height, _ = in_ref.shape
    n_y, tall, _ = out_ref.shape
    feats = tall - 8
    for y in range(n_y):
        total = in_ref[0, y * feats : (y + 1) * feats].astype(F32)
        for k in range(1, n):
            total = total + in_ref[k, y * feats : (y + 1) * feats].astype(F32)
        out_ref[y, :feats] = total.astype(BF16)
    tail = in_ref[0, height - 8 :].astype(F32)
    for k in range(1, n):
        tail = tail + in_ref[k, height - 8 :].astype(F32)
    tail = dot_rows(jnp.sum(tail, axis=0, keepdims=True)).astype(BF16)
    for y in range(n_y):
        out_ref[y, feats:] = tail


def far_body(in_ref, out_ref):
    n, tall, rows = in_ref.shape
    total = in_ref[0].astype(F32)
    for k in range(1, n):
        total = total + in_ref[k].astype(F32)
    feats = tall - 8
    tail = dot_rows(jnp.sum(total[feats:], axis=0, keepdims=True))
    rest = jnp.zeros((out_ref.shape[1] - tall, rows), F32)
    whole = jnp.concatenate([total[:feats], tail, rest], axis=0)
    out_ref[...] = whole.T.astype(BF16)


def final_body(start_ref, back_ref, dest_ref, gates_ref, tokens_ref, ratio_ref):
    rows, lanes = back_ref.shape
    feats, toks = tokens_ref.shape
    top_k, share = ratio_ref.shape
    back = back_ref[...]
    dots = back[:, feats : feats + 1].astype(F32) + back[:, feats + 1 : feats + 2].astype(F32)
    place = iota((rows, toks), 0)
    select = jnp.zeros((rows, toks), F32)
    start = start_ref[0]
    for k in range(top_k):
        at = place == dest_ref[k : k + 1, :]
        select = select + jnp.where(at, 1.0, 0.0)
        mine = jnp.sum(jnp.where(at, dots, 0.0), axis=0, keepdims=True) / gates_ref[k : k + 1, :]
        for j in range(share):
            here = iota((1, toks), 1) == start + j
            ratio_ref[k : k + 1, j : j + 1] = jnp.sum(jnp.where(here, mine, 0.0), axis=1, keepdims=True)
    summed = dot(back, select.astype(BF16), ((0,), (0,)))
    tokens_ref[...] = summed[:feats].astype(BF16)


def exchange(array, axis):
    return lax.all_to_all(array, axis, split_axis=0, concat_axis=0, tiled=True)


def on_device(tokens, out_grad, routes, gates, gate_weight, up_weight, down_weight):
    tok_dev, top_k = routes.shape
    n_ep, n_yh, n_near = lax.axis_size("ep"), lax.axis_size("yh"), lax.axis_size(NEAR)
    cap = (3 * tok_dev + n_ep - 1) // n_ep
    rows = n_ep * cap
    feats = tokens.shape[1]
    both = 2 * feats
    w_gate, w_up, w_down = gate_weight[0].T, up_weight[0].T, down_weight[0]
    hid, width = w_gate.shape

    table = jnp.zeros((2 * feats + 2 * top_k, tok_dev), F32)
    at = 0
    for a in (tokens, out_grad, routes, gates):
        table += jnp.pad(a.T, ((at, table.shape[0] - at - a.shape[1]), (0, 0))).astype(F32)
        at += a.shape[1]
    sent, dest = call(
        functools.partial(place_body, n_ep=n_ep, cap=cap, top_k=top_k),
        [((rows, both), BF16), ((top_k, tok_dev), I32)],
    )(table)
    got = exchange(sent.reshape(n_ep, cap, both), "ep").reshape(rows, both)
    (copies,) = call(turn_body, [((n_yh, both, rows), BF16)])(got)
    some = exchange(copies, "yh")
    every = exchange(jnp.broadcast_to(some[None], (n_near, *some.shape)), NEAR)

    chunks, parts = call(
        expert_body,
        [((n_near, n_yh * feats + 8, rows), BF16), ((3 * hid, rows), BF16)],
        flops=10 * hid * width * rows,
        limit=20,
    )(every, w_gate, w_up, w_down)
    swapped = exchange(chunks, NEAR)
    gate_grad, up_grad, down_grad = call(
        weights_body, [((hid, width), BF16)] * 3, flops=6 * hid * width * rows, limit=60
    )(parts, every)
    (near,) = call(near_body, [((n_yh, feats + 8, rows), BF16)])(swapped)
    (packed,) = call(far_body, [((rows, both), BF16)])(exchange(near, "yh"))
    back = exchange(packed.reshape(n_ep, cap, both), "ep").reshape(rows, both)
    share = tok_dev // (n_yh * n_near)
    start = (lax.axis_index(TP).astype(I32) * share).reshape(1)
    tokens_grad, ratio = call(
        final_body, [((feats, tok_dev), BF16), ((top_k, share), F32)], n_scalars=1
    )(start, back, dest, gates.T)
    return (
        tokens_grad.T,
        ratio.T,
        gate_grad.T[None],
        up_grad.T[None],
        down_grad[None],
    )


def solution(mesh):
    torus = Mesh(mesh.devices.reshape(mesh.shape["ep"], 4, 2, 4), ("ep", *TP))
    return jax.shard_map(
        on_device,
        mesh=torus,
        in_specs=(
            P("ep", TP),
            P("ep", TP),
            P("ep", None),
            P("ep", None),
            P("ep", None, TP),
            P("ep", None, TP),
            P("ep", TP, None),
        ),
        out_specs=(
            P("ep", TP),
            P(("ep", *TP), None),
            P("ep", None, TP),
            P("ep", None, TP),
            P("ep", TP, None),
        ),
        check_vma=False,
    )
```

```python
import functools

import jax
import jax.numpy as jnp
from jax import lax
from jax.experimental import pallas as pl
from jax.experimental.pallas import tpu as pltpu
from jax.sharding import Mesh
from jax.sharding import PartitionSpec as P

TP = ("yh", "yl", "x")
NEAR = ("yl", "x")
FAR = ("ep", "yh")
BF16 = jnp.bfloat16
F32 = jnp.float32
I32 = jnp.int32
CPU_INTERPRET = False


def call(body, outs, flops=0, n_scalars=0, limit=12):
    def run(*args):
        smem = pl.BlockSpec(memory_space=pltpu.SMEM)
        vmem = pl.BlockSpec(memory_space=pltpu.VMEM)
        size = sum(a.size * a.dtype.itemsize for a in args)
        return pl.pallas_call(
            body,
            out_shape=[jax.ShapeDtypeStruct(s, d) for s, d in outs],
            in_specs=[smem if k < n_scalars else vmem for k in range(len(args))],
            out_specs=[vmem] * len(outs),
            compiler_params=pltpu.CompilerParams(vmem_limit_bytes=limit * 2**20),
            cost_estimate=pl.CostEstimate(flops=flops, transcendentals=0, bytes_accessed=size),
            interpret=CPU_INTERPRET,
        )(*args)

    return run


def dot(a, b, dims):
    return lax.dot_general(a, b, (dims, ((), ())), preferred_element_type=F32)


def iota(shape, dim):
    return lax.broadcasted_iota(I32, shape, dim)


def dot_rows(dots):
    high = dots.astype(BF16).astype(F32)
    row = iota((8, dots.shape[1]), 0)
    return jnp.where(row == 0, high, jnp.where(row == 1, dots - high, 0.0))


def place_body(table_ref, sent_ref, dest_ref, *, n_ep, cap, top_k):
    toks = table_ref.shape[1]
    both = table_ref.shape[0] - 2 * top_k
    feats = both // 2
    routes = table_ref[both : both + top_k].astype(I32)
    gates = table_ref[both + top_k :]
    experts = -(-n_ep // 16) * 16
    hot = [(iota((experts, toks), 0) == routes[k : k + 1]).astype(BF16) for k in range(top_k)]
    hot = jnp.concatenate(hot, axis=1)
    slots = top_k * toks
    earlier = (iota((slots, slots), 0) < iota((slots, slots), 1)).astype(BF16)
    rank = jnp.sum(dot(hot, earlier, ((1,), (0,))) * hot.astype(F32), axis=0, keepdims=True)
    rank = rank.astype(I32)
    rows = n_ep * cap
    place = iota((rows, toks), 0)
    select = jnp.zeros((rows, toks), F32)
    weight = jnp.zeros((rows, 1), F32)
    for k in range(top_k):
        dest = routes[k : k + 1] * cap + rank[:, k * toks : (k + 1) * toks]
        dest_ref[k : k + 1, :] = dest
        at = place == dest
        select = select + jnp.where(at, 1.0, 0.0)
        weight = weight + jnp.sum(jnp.where(at, gates[k : k + 1], 0.0), axis=1, keepdims=True)
    moved = dot(select.astype(BF16), table_ref[:both].astype(BF16), ((1,), (1,)))
    lane = iota(moved.shape, 1)
    sent = jnp.where(lane < feats, moved, moved * weight).astype(BF16)
    for k in range(sent_ref.shape[1]):
        sent_ref[:, k] = sent.reshape(n_ep, cap, both)


def turn_body(got_ref, out_ref):
    n_ep, n_yh, cap, both = got_ref.shape
    for yh in range(n_yh):
        turned = got_ref[:, yh].reshape(n_ep * cap, both).astype(F32).T.astype(BF16)
        for k in range(out_ref.shape[0]):
            out_ref[k, yh] = turned


def column(rows_ref, yh, yl, part):
    _, _, both, _ = rows_ref.shape
    feats = both // 2
    n_x = rows_ref.shape[0] // 2
    at = slice(part * feats, (part + 1) * feats)
    return jnp.concatenate([rows_ref[yl * n_x + x, yh, at] for x in range(n_x)], axis=0)


def expert_body(rows_ref, wg_ref, wu_ref, wd_ref, out_ref, parts_ref):
    n_near, n_yh, both, _ = rows_ref.shape
    feats = both // 2
    n_x = n_near // 2
    hid = wg_ref.shape[0]
    order = [(yh, yl) for yh in range(n_yh) for yl in range(2)]
    x_t = jnp.concatenate([column(rows_ref, yh, yl, 0) for yh, yl in order], axis=0)
    pre_gate = jnp.dot(wg_ref[...], x_t, preferred_element_type=F32)
    pre_up = jnp.dot(wu_ref[...], x_t, preferred_element_type=F32)
    c_t = jnp.concatenate([column(rows_ref, yh, yl, 1) for yh, yl in order], axis=0)
    hid_grad = jnp.dot(wd_ref[...], c_t, preferred_element_type=F32)
    sig = jax.nn.sigmoid(pre_gate)
    act = pre_gate * sig
    hidden = (act * pre_up).astype(BF16)
    gate_part = (hid_grad * pre_up * sig * (1.0 + pre_gate * (1.0 - sig))).astype(BF16)
    up_part = (hid_grad * act).astype(BF16)
    dots = jnp.sum(hidden.astype(F32) * hid_grad, axis=0, keepdims=True)
    parts_ref[0:hid] = gate_part
    parts_ref[hid : 2 * hid] = up_part
    parts_ref[2 * hid : 3 * hid] = hidden
    parts = parts_ref[0 : 2 * hid]
    tail = dot_rows(dots).astype(BF16)
    for k, (yh, yl) in enumerate(order):
        cols = slice(k * n_x * feats, (k + 1) * n_x * feats)
        w = jnp.concatenate([wg_ref[:, cols], wu_ref[:, cols]], axis=0)
        piece = dot(w, parts, ((0,), (0,))).astype(BF16)
        for x in range(n_x):
            at = slice(yh * feats, (yh + 1) * feats)
            out_ref[yl * n_x + x, at] = piece[x * feats : (x + 1) * feats]
    for k in range(n_near):
        out_ref[k, n_yh * feats :] = tail


def weights_body(parts_ref, rows_ref, gate_ref, up_ref, down_ref):
    n_near, n_yh, both, _ = rows_ref.shape
    wide = n_near // 2 * (both // 2)
    hid = gate_ref.shape[0]
    for yh in range(n_yh):
        for yl in range(2):
            k = 2 * yh + yl
            cols = slice(k * wide, (k + 1) * wide)
            x_t, c_t = column(rows_ref, yh, yl, 0), column(rows_ref, yh, yl, 1)
            grads = dot(parts_ref[0 : 2 * hid], x_t, ((1,), (1,))).astype(BF16)
            gate_ref[:, cols] = grads[:hid]
            up_ref[:, cols] = grads[hid:]
            down_ref[:, cols] = dot(parts_ref[2 * hid :], c_t, ((1,), (1,))).astype(BF16)


def sum_body(in_ref, out_ref):
    n, height, rows = in_ref.shape
    n_ep, n_yh, cap, both = out_ref.shape
    feats = both // 2

    def total(at):
        whole = in_ref[0, at].astype(F32)
        for k in range(1, n):
            whole = whole + in_ref[k, at].astype(F32)
        return whole

    tail = total(slice(n_yh * feats, height))
    tail = dot_rows(jnp.sum(tail, axis=0, keepdims=True))
    rest = jnp.zeros((both - feats - 8, rows), F32)
    for yh in range(n_yh):
        block = total(slice(yh * feats, (yh + 1) * feats))
        turned = jnp.concatenate([block, tail, rest], axis=0).T
        out_ref[:, yh] = turned.astype(BF16).reshape(n_ep, cap, both)


def final_body(start_ref, back_ref, dest_ref, gates_ref, tokens_ref, ratio_ref):
    n_ep, n_yh, cap, both = back_ref.shape
    rows = n_ep * cap
    feats, toks = tokens_ref.shape
    top_k, share = ratio_ref.shape
    back = back_ref[:, 0].astype(F32)
    for yh in range(1, n_yh):
        back = back + back_ref[:, yh].astype(F32)
    back = back.reshape(rows, both)
    dots = back[:, feats : feats + 1] + back[:, feats + 1 : feats + 2]
    place = iota((rows, toks), 0)
    select = jnp.zeros((rows, toks), F32)
    start = start_ref[0]
    for k in range(top_k):
        at = place == dest_ref[k : k + 1, :]
        select = select + jnp.where(at, 1.0, 0.0)
        mine = jnp.sum(jnp.where(at, dots, 0.0), axis=0, keepdims=True) / gates_ref[k : k + 1, :]
        for j in range(share):
            here = iota((1, toks), 1) == start + j
            ratio_ref[k : k + 1, j : j + 1] = jnp.sum(jnp.where(here, mine, 0.0), axis=1, keepdims=True)
    high = back.astype(BF16)
    low = (back - high.astype(F32)).astype(BF16)
    select = select.astype(BF16)
    summed = dot(high, select, ((0,), (0,))) + dot(low, select, ((0,), (0,)))
    tokens_ref[...] = summed[:feats].astype(BF16)


def exchange(array, axis):
    return lax.all_to_all(array, axis, split_axis=0, concat_axis=0, tiled=True)


def on_device(tokens, out_grad, routes, gates, gate_weight, up_weight, down_weight):
    tok_dev, top_k = routes.shape
    n_ep, n_yh, n_near = lax.axis_size("ep"), lax.axis_size("yh"), lax.axis_size(NEAR)
    cap = (3 * tok_dev + n_ep - 1) // n_ep
    rows = n_ep * cap
    feats = tokens.shape[1]
    both = 2 * feats
    w_gate, w_up, w_down = gate_weight[0].T, up_weight[0].T, down_weight[0]
    hid, width = w_gate.shape

    table = jnp.zeros((2 * feats + 2 * top_k, tok_dev), F32)
    at = 0
    for a in (tokens, out_grad, routes, gates):
        table += jnp.pad(a.T, ((at, table.shape[0] - at - a.shape[1]), (0, 0))).astype(F32)
        at += a.shape[1]
    sent, dest = call(
        functools.partial(place_body, n_ep=n_ep, cap=cap, top_k=top_k),
        [((n_ep, n_yh, cap, both), BF16), ((top_k, tok_dev), I32)],
    )(table)
    got = exchange(sent.reshape(n_ep * n_yh, cap, both), FAR).reshape(n_ep, n_yh, cap, both)
    (copies,) = call(turn_body, [((n_near, n_yh, both, rows), BF16)])(got)
    every = exchange(copies, NEAR)

    chunks, parts = call(
        expert_body,
        [((n_near, n_yh * feats + 8, rows), BF16), ((3 * hid, rows), BF16)],
        flops=10 * hid * width * rows,
        limit=20,
    )(every, w_gate, w_up, w_down)
    swapped = exchange(chunks, NEAR)
    gate_grad, up_grad, down_grad = call(
        weights_body, [((hid, width), BF16)] * 3, flops=6 * hid * width * rows, limit=60
    )(parts, every)
    (packed,) = call(sum_body, [((n_ep, n_yh, cap, both), BF16)])(swapped)
    back = exchange(packed.reshape(n_ep * n_yh, cap, both), FAR).reshape(n_ep, n_yh, cap, both)
    share = tok_dev // (n_yh * n_near)
    start = (lax.axis_index(TP).astype(I32) * share).reshape(1)
    tokens_grad, ratio = call(
        final_body, [((feats, tok_dev), BF16), ((top_k, share), F32)], n_scalars=1
    )(start, back, dest, gates.T)
    return (
        tokens_grad.T,
        ratio.T,
        gate_grad.T[None],
        up_grad.T[None],
        down_grad[None],
    )


def solution(mesh):
    torus = Mesh(mesh.devices.reshape(mesh.shape["ep"], 4, 2, 4), ("ep", *TP))
    return jax.shard_map(
        on_device,
        mesh=torus,
        in_specs=(
            P("ep", TP),
            P("ep", TP),
            P("ep", None),
            P("ep", None),
            P("ep", None, TP),
            P("ep", None, TP),
            P("ep", TP, None),
        ),
        out_specs=(
            P("ep", TP),
            P(("ep", *TP), None),
            P("ep", None, TP),
            P("ep", None, TP),
            P("ep", TP, None),
        ),
        check_vma=False,
    )
```

```python
import functools

import jax
import jax.numpy as jnp
from jax import lax
from jax.experimental import pallas as pl
from jax.experimental.pallas import tpu as pltpu
from jax.sharding import Mesh
from jax.sharding import PartitionSpec as P

TP = ("yh", "yl", "xh", "xl")
FAR = ("yh", "xh")
BF16 = jnp.bfloat16
F32 = jnp.float32
I32 = jnp.int32
CPU_INTERPRET = False


def call(body, outs, flops=0, n_scalars=0, limit=12):
    def run(*args):
        smem = pl.BlockSpec(memory_space=pltpu.SMEM)
        vmem = pl.BlockSpec(memory_space=pltpu.VMEM)
        size = sum(a.size * a.dtype.itemsize for a in args)
        return pl.pallas_call(
            body,
            out_shape=[jax.ShapeDtypeStruct(s, d) for s, d in outs],
            in_specs=[smem if k < n_scalars else vmem for k in range(len(args))],
            out_specs=[vmem] * len(outs),
            compiler_params=pltpu.CompilerParams(vmem_limit_bytes=limit * 2**20),
            cost_estimate=pl.CostEstimate(flops=flops, transcendentals=0, bytes_accessed=size),
            interpret=CPU_INTERPRET,
        )(*args)

    return run


def dot(a, b, dims):
    return lax.dot_general(a, b, (dims, ((), ())), preferred_element_type=F32)


def iota(shape, dim):
    return lax.broadcasted_iota(I32, shape, dim)


def dot_rows(dots):
    high = dots.astype(BF16).astype(F32)
    row = iota((8, dots.shape[1]), 0)
    return jnp.where(row == 0, high, jnp.where(row == 1, dots - high, 0.0))


def place_body(table_ref, sent_ref, dest_ref, *, n_ep, cap, top_k):
    toks = table_ref.shape[1]
    both = table_ref.shape[0] - 2 * top_k
    feats = both // 2
    routes = table_ref[both : both + top_k].astype(I32)
    gates = table_ref[both + top_k :]
    experts = -(-n_ep // 16) * 16
    hot = [(iota((experts, toks), 0) == routes[k : k + 1]).astype(BF16) for k in range(top_k)]
    hot = jnp.concatenate(hot, axis=1)
    slots = top_k * toks
    earlier = (iota((slots, slots), 0) < iota((slots, slots), 1)).astype(BF16)
    rank = jnp.sum(dot(hot, earlier, ((1,), (0,))) * hot.astype(F32), axis=0, keepdims=True)
    rank = rank.astype(I32)
    rows = n_ep * cap
    place = iota((rows, toks), 0)
    select = jnp.zeros((rows, toks), F32)
    weight = jnp.zeros((rows, 1), F32)
    for k in range(top_k):
        dest = routes[k : k + 1] * cap + rank[:, k * toks : (k + 1) * toks]
        dest_ref[k : k + 1, :] = dest
        at = place == dest
        select = select + jnp.where(at, 1.0, 0.0)
        weight = weight + jnp.sum(jnp.where(at, gates[k : k + 1], 0.0), axis=1, keepdims=True)
    moved = dot(select.astype(BF16), table_ref[:both].astype(BF16), ((1,), (1,)))
    lane = iota(moved.shape, 1)
    sent_ref[...] = jnp.where(lane < feats, moved, moved * weight).astype(BF16)


def turn_body(got_ref, out_ref):
    turned = got_ref[...].astype(F32).T.astype(BF16)
    for k in range(out_ref.shape[0]):
        out_ref[k] = turned


def column(rows_ref, yh, yl, part):
    feats = rows_ref.shape[2] // 2
    at = slice(part * feats, (part + 1) * feats)
    return jnp.concatenate(
        [rows_ref[yl * 2 + xl, yh * 2 + xh, at] for xh in range(2) for xl in range(2)], axis=0
    )


def expert_body(rows_ref, wg_ref, wu_ref, wd_ref, out_ref, parts_ref):
    n_near, n_far, both, _ = rows_ref.shape
    n_yh = n_far // 2
    feats = both // 2
    n_x = 4
    hid = wg_ref.shape[0]
    order = [(yh, yl) for yh in range(n_yh) for yl in range(2)]
    x_t = jnp.concatenate([column(rows_ref, yh, yl, 0) for yh, yl in order], axis=0)
    pre_gate = jnp.dot(wg_ref[...], x_t, preferred_element_type=F32)
    pre_up = jnp.dot(wu_ref[...], x_t, preferred_element_type=F32)
    c_t = jnp.concatenate([column(rows_ref, yh, yl, 1) for yh, yl in order], axis=0)
    hid_grad = jnp.dot(wd_ref[...], c_t, preferred_element_type=F32)
    sig = jax.nn.sigmoid(pre_gate)
    act = pre_gate * sig
    hidden = (act * pre_up).astype(BF16)
    gate_part = (hid_grad * pre_up * sig * (1.0 + pre_gate * (1.0 - sig))).astype(BF16)
    up_part = (hid_grad * act).astype(BF16)
    dots = jnp.sum(hidden.astype(F32) * hid_grad, axis=0, keepdims=True)
    parts_ref[0:hid] = gate_part
    parts_ref[hid : 2 * hid] = up_part
    parts_ref[2 * hid : 3 * hid] = hidden
    parts = parts_ref[0 : 2 * hid]
    tail = dot_rows(dots).astype(BF16)
    for k, (yh, yl) in enumerate(order):
        cols = slice(k * n_x * feats, (k + 1) * n_x * feats)
        w = jnp.concatenate([wg_ref[:, cols], wu_ref[:, cols]], axis=0)
        piece = dot(w, parts, ((0,), (0,))).astype(BF16)
        for x in range(n_x):
            at = (yh * 2 + x // 2) * feats
            out_ref[yl * 2 + x % 2, at : at + feats] = piece[x * feats : (x + 1) * feats]
    for k in range(n_near):
        out_ref[k, n_far * feats :] = tail


def weights_body(parts_ref, rows_ref, gate_ref, up_ref, down_ref):
    n_yh = rows_ref.shape[1] // 2
    wide = 4 * (rows_ref.shape[2] // 2)
    hid = gate_ref.shape[0]
    for yh in range(n_yh):
        for yl in range(2):
            k = 2 * yh + yl
            cols = slice(k * wide, (k + 1) * wide)
            x_t, c_t = column(rows_ref, yh, yl, 0), column(rows_ref, yh, yl, 1)
            grads = dot(parts_ref[0 : 2 * hid], x_t, ((1,), (1,))).astype(BF16)
            gate_ref[:, cols] = grads[:hid]
            up_ref[:, cols] = grads[hid:]
            down_ref[:, cols] = dot(parts_ref[2 * hid :], c_t, ((1,), (1,))).astype(BF16)


def near_body(in_ref, out_ref):
    n, height, _ = in_ref.shape
    n_y, tall, _ = out_ref.shape
    feats = tall - 8
    for y in range(n_y):
        total = in_ref[0, y * feats : (y + 1) * feats].astype(F32)
        for k in range(1, n):
            total = total + in_ref[k, y * feats : (y + 1) * feats].astype(F32)
        out_ref[y, :feats] = total.astype(BF16)
    tail = in_ref[0, height - 8 :].astype(F32)
    for k in range(1, n):
        tail = tail + in_ref[k, height - 8 :].astype(F32)
    tail = dot_rows(jnp.sum(tail, axis=0, keepdims=True)).astype(BF16)
    for y in range(n_y):
        out_ref[y, feats:] = tail


def far_body(in_ref, out_ref):
    n, tall, rows = in_ref.shape
    total = in_ref[0].astype(F32)
    for k in range(1, n):
        total = total + in_ref[k].astype(F32)
    feats = tall - 8
    tail = dot_rows(jnp.sum(total[feats:], axis=0, keepdims=True))
    rest = jnp.zeros((out_ref.shape[1] - tall, rows), F32)
    whole = jnp.concatenate([total[:feats], tail, rest], axis=0)
    out_ref[...] = whole.T.astype(BF16)


def final_body(start_ref, back_ref, dest_ref, gates_ref, tokens_ref, ratio_ref):
    rows, lanes = back_ref.shape
    feats, toks = tokens_ref.shape
    top_k, share = ratio_ref.shape
    back = back_ref[...]
    dots = back[:, feats : feats + 1].astype(F32) + back[:, feats + 1 : feats + 2].astype(F32)
    place = iota((rows, toks), 0)
    select = jnp.zeros((rows, toks), F32)
    start = start_ref[0]
    for k in range(top_k):
        at = place == dest_ref[k : k + 1, :]
        select = select + jnp.where(at, 1.0, 0.0)
        mine = jnp.sum(jnp.where(at, dots, 0.0), axis=0, keepdims=True) / gates_ref[k : k + 1, :]
        for j in range(share):
            here = iota((1, toks), 1) == start + j
            ratio_ref[k : k + 1, j : j + 1] = jnp.sum(jnp.where(here, mine, 0.0), axis=1, keepdims=True)
    summed = dot(back, select.astype(BF16), ((0,), (0,)))
    tokens_ref[...] = summed[:feats].astype(BF16)


def exchange(array, axis, groups=None):
    return lax.all_to_all(
        array, axis, split_axis=0, concat_axis=0, tiled=True, axis_index_groups=groups
    )


def neighbours(n_ep, n_y, n_x):
    groups = []
    for ep in range(n_ep):
        step = 2 * (ep % 2)
        for y in range(1, n_y, 2):
            for x in range(1, n_x, 2):
                ys, xs = ((y - 1 + step) % n_y, y), ((x - 1 + step) % n_x, x)
                groups.append([(ep * n_y + i) * n_x + j for i in ys for j in xs])
    return groups


def on_device(tokens, out_grad, routes, gates, gate_weight, up_weight, down_weight):
    tok_dev, top_k = routes.shape
    n_ep, n_far, n_near = lax.axis_size("ep"), lax.axis_size(FAR), 4
    whole = ("ep", *TP)
    blocks = neighbours(n_ep, 2 * lax.axis_size("yh"), 2 * lax.axis_size("xh"))
    cap = (3 * tok_dev + n_ep - 1) // n_ep
    rows = n_ep * cap
    feats = tokens.shape[1]
    both = 2 * feats
    w_gate, w_up, w_down = gate_weight[0].T, up_weight[0].T, down_weight[0]
    hid, width = w_gate.shape

    table = jnp.zeros((2 * feats + 2 * top_k, tok_dev), F32)
    at = 0
    for a in (tokens, out_grad, routes, gates):
        table += jnp.pad(a.T, ((at, table.shape[0] - at - a.shape[1]), (0, 0))).astype(F32)
        at += a.shape[1]
    sent, dest = call(
        functools.partial(place_body, n_ep=n_ep, cap=cap, top_k=top_k),
        [((rows, both), BF16), ((top_k, tok_dev), I32)],
    )(table)
    got = exchange(sent.reshape(n_ep, cap, both), "ep").reshape(rows, both)
    (copies,) = call(turn_body, [((n_far, both, rows), BF16)])(got)
    some = exchange(copies, FAR)
    every = exchange(jnp.broadcast_to(some[None], (n_near, *some.shape)), whole, blocks)

    chunks, parts = call(
        expert_body,
        [((n_near, n_far * feats + 8, rows), BF16), ((3 * hid, rows), BF16)],
        flops=10 * hid * width * rows,
        limit=20,
    )(every, w_gate, w_up, w_down)
    swapped = exchange(chunks, whole, blocks)
    gate_grad, up_grad, down_grad = call(
        weights_body, [((hid, width), BF16)] * 3, flops=6 * hid * width * rows, limit=60
    )(parts, every)
    (near,) = call(near_body, [((n_far, feats + 8, rows), BF16)])(swapped)
    (packed,) = call(far_body, [((rows, both), BF16)])(exchange(near, FAR))
    back = exchange(packed.reshape(n_ep, cap, both), "ep").reshape(rows, both)
    share = tok_dev // (n_far * n_near)
    start = (lax.axis_index(TP).astype(I32) * share).reshape(1)
    tokens_grad, ratio = call(
        final_body, [((feats, tok_dev), BF16), ((top_k, share), F32)], n_scalars=1
    )(start, back, dest, gates.T)
    return (
        tokens_grad.T,
        ratio.T,
        gate_grad.T[None],
        up_grad.T[None],
        down_grad[None],
    )


def solution(mesh):
    torus = Mesh(mesh.devices.reshape(mesh.shape["ep"], 4, 2, 2, 2), ("ep", *TP))
    return jax.shard_map(
        on_device,
        mesh=torus,
        in_specs=(
            P("ep", TP),
            P("ep", TP),
            P("ep", None),
            P("ep", None),
            P("ep", None, TP),
            P("ep", None, TP),
            P("ep", TP, None),
        ),
        out_specs=(
            P("ep", TP),
            P(("ep", *TP), None),
            P("ep", None, TP),
            P("ep", None, TP),
            P("ep", TP, None),
        ),
        check_vma=False,
    )
```

```python
import functools

import jax
import jax.numpy as jnp
from jax import lax
from jax.experimental import pallas as pl
from jax.experimental.pallas import tpu as pltpu
from jax.sharding import Mesh
from jax.sharding import PartitionSpec as P

TP = ("ya", "yb", "yl", "xh", "xl")
FIRST = ("ep", "ya")
SECOND = ("yb", "xh")
FAR = ("ya", "yb", "xh")
BF16 = jnp.bfloat16
F32 = jnp.float32
I32 = jnp.int32
CPU_INTERPRET = False


def call(body, outs, flops=0, n_scalars=0, limit=12):
    def run(*args):
        smem = pl.BlockSpec(memory_space=pltpu.SMEM)
        vmem = pl.BlockSpec(memory_space=pltpu.VMEM)
        size = sum(a.size * a.dtype.itemsize for a in args)
        return pl.pallas_call(
            body,
            out_shape=[jax.ShapeDtypeStruct(s, d) for s, d in outs],
            in_specs=[smem if k < n_scalars else vmem for k in range(len(args))],
            out_specs=[vmem] * len(outs),
            compiler_params=pltpu.CompilerParams(vmem_limit_bytes=limit * 2**20),
            cost_estimate=pl.CostEstimate(flops=flops, transcendentals=0, bytes_accessed=size),
            interpret=CPU_INTERPRET,
        )(*args)

    return run


def dot(a, b, dims):
    return lax.dot_general(a, b, (dims, ((), ())), preferred_element_type=F32)


def iota(shape, dim):
    return lax.broadcasted_iota(I32, shape, dim)


def dot_rows(dots):
    high = dots.astype(BF16).astype(F32)
    row = iota((8, dots.shape[1]), 0)
    return jnp.where(row == 0, high, jnp.where(row == 1, dots - high, 0.0))


def place_body(table_ref, sent_ref, dest_ref, *, n_ep, cap, top_k):
    toks = table_ref.shape[1]
    both = table_ref.shape[0] - 2 * top_k
    feats = both // 2
    routes = table_ref[both : both + top_k].astype(I32)
    gates = table_ref[both + top_k :]
    experts = -(-n_ep // 16) * 16
    hot = [(iota((experts, toks), 0) == routes[k : k + 1]).astype(BF16) for k in range(top_k)]
    hot = jnp.concatenate(hot, axis=1)
    slots = top_k * toks
    earlier = (iota((slots, slots), 0) < iota((slots, slots), 1)).astype(BF16)
    rank = jnp.sum(dot(hot, earlier, ((1,), (0,))) * hot.astype(F32), axis=0, keepdims=True)
    rank = rank.astype(I32)
    rows = n_ep * cap
    place = iota((rows, toks), 0)
    select = jnp.zeros((rows, toks), F32)
    weight = jnp.zeros((rows, 1), F32)
    for k in range(top_k):
        dest = routes[k : k + 1] * cap + rank[:, k * toks : (k + 1) * toks]
        dest_ref[k : k + 1, :] = dest
        at = place == dest
        select = select + jnp.where(at, 1.0, 0.0)
        weight = weight + jnp.sum(jnp.where(at, gates[k : k + 1], 0.0), axis=1, keepdims=True)
    moved = dot(select.astype(BF16), table_ref[:both].astype(BF16), ((1,), (1,)))
    lane = iota(moved.shape, 1)
    sent = jnp.where(lane < feats, moved, moved * weight).astype(BF16)
    for k in range(sent_ref.shape[1]):
        sent_ref[:, k] = sent.reshape(n_ep, cap, both)


def turn_body(got_ref, out_ref):
    n_ep, n_ya, cap, both = got_ref.shape
    for ya in range(n_ya):
        turned = got_ref[:, ya].reshape(n_ep * cap, both).astype(F32).T.astype(BF16)
        for k in range(out_ref.shape[0]):
            out_ref[k, ya] = turned


def column(rows_ref, yh, yl, part):
    feats = rows_ref.shape[3] // 2
    n_yb = rows_ref.shape[1] // 2
    ya, yb = yh // n_yb, yh % n_yb
    at = slice(part * feats, (part + 1) * feats)
    return jnp.concatenate(
        [rows_ref[yl * 2 + xl, yb * 2 + xh, ya, at] for xh in range(2) for xl in range(2)], axis=0
    )


def expert_body(rows_ref, wg_ref, wu_ref, wd_ref, out_ref, parts_ref):
    n_near, n_second, n_ya, both, _ = rows_ref.shape
    n_far = n_second * n_ya
    n_yh = n_far // 2
    feats = both // 2
    n_x = 4
    hid = wg_ref.shape[0]
    order = [(yh, yl) for yh in range(n_yh) for yl in range(2)]
    x_t = jnp.concatenate([column(rows_ref, yh, yl, 0) for yh, yl in order], axis=0)
    pre_gate = jnp.dot(wg_ref[...], x_t, preferred_element_type=F32)
    pre_up = jnp.dot(wu_ref[...], x_t, preferred_element_type=F32)
    c_t = jnp.concatenate([column(rows_ref, yh, yl, 1) for yh, yl in order], axis=0)
    hid_grad = jnp.dot(wd_ref[...], c_t, preferred_element_type=F32)
    sig = jax.nn.sigmoid(pre_gate)
    act = pre_gate * sig
    hidden = (act * pre_up).astype(BF16)
    gate_part = (hid_grad * pre_up * sig * (1.0 + pre_gate * (1.0 - sig))).astype(BF16)
    up_part = (hid_grad * act).astype(BF16)
    dots = jnp.sum(hidden.astype(F32) * hid_grad, axis=0, keepdims=True)
    parts_ref[0:hid] = gate_part
    parts_ref[hid : 2 * hid] = up_part
    parts_ref[2 * hid : 3 * hid] = hidden
    parts = parts_ref[0 : 2 * hid]
    tail = dot_rows(dots).astype(BF16)
    for k, (yh, yl) in enumerate(order):
        cols = slice(k * n_x * feats, (k + 1) * n_x * feats)
        w = jnp.concatenate([wg_ref[:, cols], wu_ref[:, cols]], axis=0)
        piece = dot(w, parts, ((0,), (0,))).astype(BF16)
        for x in range(n_x):
            at = (yh * 2 + x // 2) * feats
            out_ref[yl * 2 + x % 2, at : at + feats] = piece[x * feats : (x + 1) * feats]
    for k in range(n_near):
        out_ref[k, n_far * feats :] = tail


def weights_body(parts_ref, rows_ref, gate_ref, up_ref, down_ref):
    n_yh = rows_ref.shape[1] * rows_ref.shape[2] // 2
    wide = 4 * (rows_ref.shape[3] // 2)
    hid = gate_ref.shape[0]
    for yh in range(n_yh):
        for yl in range(2):
            k = 2 * yh + yl
            cols = slice(k * wide, (k + 1) * wide)
            x_t, c_t = column(rows_ref, yh, yl, 0), column(rows_ref, yh, yl, 1)
            grads = dot(parts_ref[0 : 2 * hid], x_t, ((1,), (1,))).astype(BF16)
            gate_ref[:, cols] = grads[:hid]
            up_ref[:, cols] = grads[hid:]
            down_ref[:, cols] = dot(parts_ref[2 * hid :], c_t, ((1,), (1,))).astype(BF16)


def near_body(in_ref, out_ref):
    n, height, _ = in_ref.shape
    n_y, tall, _ = out_ref.shape
    feats = tall - 8
    for y in range(n_y):
        total = in_ref[0, y * feats : (y + 1) * feats].astype(F32)
        for k in range(1, n):
            total = total + in_ref[k, y * feats : (y + 1) * feats].astype(F32)
        out_ref[y, :feats] = total.astype(BF16)
    tail = in_ref[0, height - 8 :].astype(F32)
    for k in range(1, n):
        tail = tail + in_ref[k, height - 8 :].astype(F32)
    tail = dot_rows(jnp.sum(tail, axis=0, keepdims=True)).astype(BF16)
    for y in range(n_y):
        out_ref[y, feats:] = tail


def far_body(in_ref, out_ref):
    n, tall, rows = in_ref.shape
    total = in_ref[0].astype(F32)
    for k in range(1, n):
        total = total + in_ref[k].astype(F32)
    feats = tall - 8
    tail = dot_rows(jnp.sum(total[feats:], axis=0, keepdims=True))
    rest = jnp.zeros((out_ref.shape[1] - tall, rows), F32)
    whole = jnp.concatenate([total[:feats], tail, rest], axis=0)
    out_ref[...] = whole.T.astype(BF16)


def final_body(start_ref, back_ref, dest_ref, gates_ref, tokens_ref, ratio_ref):
    rows, lanes = back_ref.shape
    feats, toks = tokens_ref.shape
    top_k, share = ratio_ref.shape
    back = back_ref[...]
    dots = back[:, feats : feats + 1].astype(F32) + back[:, feats + 1 : feats + 2].astype(F32)
    place = iota((rows, toks), 0)
    select = jnp.zeros((rows, toks), F32)
    start = start_ref[0]
    for k in range(top_k):
        at = place == dest_ref[k : k + 1, :]
        select = select + jnp.where(at, 1.0, 0.0)
        mine = jnp.sum(jnp.where(at, dots, 0.0), axis=0, keepdims=True) / gates_ref[k : k + 1, :]
        for j in range(share):
            here = iota((1, toks), 1) == start + j
            ratio_ref[k : k + 1, j : j + 1] = jnp.sum(jnp.where(here, mine, 0.0), axis=1, keepdims=True)
    summed = dot(back, select.astype(BF16), ((0,), (0,)))
    tokens_ref[...] = summed[:feats].astype(BF16)


def exchange(array, axis, groups=None):
    return lax.all_to_all(
        array, axis, split_axis=0, concat_axis=0, tiled=True, axis_index_groups=groups
    )


def neighbours(n_ep, n_y, n_x):
    groups = []
    for ep in range(n_ep):
        step = 2 * (ep % 2)
        for y in range(1, n_y, 2):
            for x in range(1, n_x, 2):
                ys, xs = ((y - 1 + step) % n_y, y), ((x - 1 + step) % n_x, x)
                groups.append([(ep * n_y + i) * n_x + j for i in ys for j in xs])
    return groups


def second_groups(n_ep, n_y, n_x):
    groups = []
    for ep in range(n_ep):
        for a in range(0, n_y, 4):
            for yl in range(2):
                ys = ((a + 4 * (ep % 2)) % n_y + yl, a + 2 + yl)
                for xl in range(2):
                    xs = (xl, xl + 2)
                    groups.append([(ep * n_y + i) * n_x + j for i in ys for j in xs])
    return groups


def on_device(tokens, out_grad, routes, gates, gate_weight, up_weight, down_weight):
    tok_dev, top_k = routes.shape
    n_ep, n_far, n_near = lax.axis_size("ep"), lax.axis_size(FAR), 4
    whole = ("ep", *TP)
    blocks = neighbours(n_ep, lax.axis_size(("ya", "yb", "yl")), 2 * lax.axis_size("xh"))
    n_ya, n_second = lax.axis_size("ya"), lax.axis_size(SECOND)
    pairs = second_groups(n_ep, lax.axis_size(("ya", "yb", "yl")), 2 * lax.axis_size("xh"))
    cap = (3 * tok_dev + n_ep - 1) // n_ep
    rows = n_ep * cap
    feats = tokens.shape[1]
    both = 2 * feats
    w_gate, w_up, w_down = gate_weight[0].T, up_weight[0].T, down_weight[0]
    hid, width = w_gate.shape

    table = jnp.zeros((2 * feats + 2 * top_k, tok_dev), F32)
    at = 0
    for a in (tokens, out_grad, routes, gates):
        table += jnp.pad(a.T, ((at, table.shape[0] - at - a.shape[1]), (0, 0))).astype(F32)
        at += a.shape[1]
    sent, dest = call(
        functools.partial(place_body, n_ep=n_ep, cap=cap, top_k=top_k),
        [((n_ep, n_ya, cap, both), BF16), ((top_k, tok_dev), I32)],
    )(table)
    got = exchange(sent.reshape(n_ep * n_ya, cap, both), FIRST).reshape(n_ep, n_ya, cap, both)
    (copies,) = call(turn_body, [((n_second, n_ya, both, rows), BF16)])(got)
    some = exchange(copies, whole, pairs)
    every = exchange(jnp.broadcast_to(some[None], (n_near, *some.shape)), whole, blocks)

    chunks, parts = call(
        expert_body,
        [((n_near, n_far * feats + 8, rows), BF16), ((3 * hid, rows), BF16)],
        flops=10 * hid * width * rows,
        limit=20,
    )(every, w_gate, w_up, w_down)
    swapped = exchange(chunks, whole, blocks)
    gate_grad, up_grad, down_grad = call(
        weights_body, [((hid, width), BF16)] * 3, flops=6 * hid * width * rows, limit=60
    )(parts, every)
    (near,) = call(near_body, [((n_far, feats + 8, rows), BF16)])(swapped)
    (packed,) = call(far_body, [((rows, both), BF16)])(exchange(near, FAR))
    back = exchange(packed.reshape(n_ep, cap, both), "ep").reshape(rows, both)
    share = tok_dev // (n_far * n_near)
    start = (lax.axis_index(TP).astype(I32) * share).reshape(1)
    tokens_grad, ratio = call(
        final_body, [((feats, tok_dev), BF16), ((top_k, share), F32)], n_scalars=1
    )(start, back, dest, gates.T)
    return (
        tokens_grad.T,
        ratio.T,
        gate_grad.T[None],
        up_grad.T[None],
        down_grad[None],
    )


def solution(mesh):
    torus = Mesh(mesh.devices.reshape(mesh.shape["ep"], 2, 2, 2, 2, 2), ("ep", *TP))
    return jax.shard_map(
        on_device,
        mesh=torus,
        in_specs=(
            P("ep", TP),
            P("ep", TP),
            P("ep", None),
            P("ep", None),
            P("ep", None, TP),
            P("ep", None, TP),
            P("ep", TP, None),
        ),
        out_specs=(
            P("ep", TP),
            P(("ep", *TP), None),
            P("ep", None, TP),
            P("ep", None, TP),
            P("ep", TP, None),
        ),
        check_vma=False,
    )
```

```python
import functools

import jax
import jax.numpy as jnp
from jax import lax
from jax.experimental import pallas as pl
from jax.experimental.pallas import tpu as pltpu
from jax.sharding import Mesh
from jax.sharding import PartitionSpec as P

TP = ("ya", "yb", "yl", "xh", "xl")
FIRST = ("ep", "ya")
SECOND = ("yb", "xh")
FAR = ("ya", "yb", "xh")
BF16 = jnp.bfloat16
F32 = jnp.float32
I32 = jnp.int32
CPU_INTERPRET = False


def call(body, outs, flops=0, n_scalars=0, limit=12):
    def run(*args):
        smem = pl.BlockSpec(memory_space=pltpu.SMEM)
        vmem = pl.BlockSpec(memory_space=pltpu.VMEM)
        size = sum(a.size * a.dtype.itemsize for a in args)
        return pl.pallas_call(
            body,
            out_shape=[jax.ShapeDtypeStruct(s, d) for s, d in outs],
            in_specs=[smem if k < n_scalars else vmem for k in range(len(args))],
            out_specs=[vmem] * len(outs),
            compiler_params=pltpu.CompilerParams(vmem_limit_bytes=limit * 2**20),
            cost_estimate=pl.CostEstimate(flops=flops, transcendentals=0, bytes_accessed=size),
            interpret=CPU_INTERPRET,
        )(*args)

    return run


def dot(a, b, dims):
    return lax.dot_general(a, b, (dims, ((), ())), preferred_element_type=F32)


def iota(shape, dim):
    return lax.broadcasted_iota(I32, shape, dim)


def dot_rows(dots):
    high = dots.astype(BF16).astype(F32)
    row = iota((8, dots.shape[1]), 0)
    return jnp.where(row == 0, high, jnp.where(row == 1, dots - high, 0.0))


def place_body(table_ref, sent_ref, dest_ref, *, n_ep, cap, top_k):
    toks = table_ref.shape[1]
    both = table_ref.shape[0] - 2 * top_k
    feats = both // 2
    routes = table_ref[both : both + top_k].astype(I32)
    gates = table_ref[both + top_k :]
    experts = -(-n_ep // 16) * 16
    hot = [(iota((experts, toks), 0) == routes[k : k + 1]).astype(BF16) for k in range(top_k)]
    hot = jnp.concatenate(hot, axis=1)
    slots = top_k * toks
    earlier = (iota((slots, slots), 0) < iota((slots, slots), 1)).astype(BF16)
    rank = jnp.sum(dot(hot, earlier, ((1,), (0,))) * hot.astype(F32), axis=0, keepdims=True)
    rank = rank.astype(I32)
    rows = n_ep * cap
    place = iota((rows, toks), 0)
    select = jnp.zeros((rows, toks), F32)
    weight = jnp.zeros((rows, 1), F32)
    for k in range(top_k):
        dest = routes[k : k + 1] * cap + rank[:, k * toks : (k + 1) * toks]
        dest_ref[k : k + 1, :] = dest
        at = place == dest
        select = select + jnp.where(at, 1.0, 0.0)
        weight = weight + jnp.sum(jnp.where(at, gates[k : k + 1], 0.0), axis=1, keepdims=True)
    moved = dot(select.astype(BF16), table_ref[:both].astype(BF16), ((1,), (1,)))
    lane = iota(moved.shape, 1)
    sent = jnp.where(lane < feats, moved, moved * weight).astype(BF16)
    for k in range(sent_ref.shape[1]):
        sent_ref[:, k] = sent.reshape(n_ep, cap, both)


def turn_body(got_ref, out_ref):
    n_ep, n_ya, cap, both = got_ref.shape
    for ya in range(n_ya):
        turned = got_ref[:, ya].reshape(n_ep * cap, both).astype(F32).T.astype(BF16)
        for k in range(out_ref.shape[0]):
            out_ref[k, ya] = turned


def around(i, j):
    return 2 * i + (i ^ j)


def circle(ys, xs, ep, n_y, n_x):
    corners = ((0, 0), (0, 1), (1, 1), (1, 0))
    return [(ep * n_y + ys[i]) * n_x + xs[j] for i, j in corners]


def column(rows_ref, yh, yl, part):
    feats = rows_ref.shape[3] // 2
    n_yb = rows_ref.shape[1] // 2
    ya, yb = yh // n_yb, yh % n_yb
    at = slice(part * feats, (part + 1) * feats)
    return jnp.concatenate(
        [rows_ref[around(yl, xl), around(yb, xh), ya, at] for xh in range(2) for xl in range(2)], axis=0
    )


def expert_body(rows_ref, wg_ref, wu_ref, wd_ref, out_ref, parts_ref):
    n_near, n_second, n_ya, both, _ = rows_ref.shape
    n_far = n_second * n_ya
    n_yh = n_far // 2
    feats = both // 2
    n_x = 4
    hid = wg_ref.shape[0]
    order = [(yh, yl) for yh in range(n_yh) for yl in range(2)]
    x_t = jnp.concatenate([column(rows_ref, yh, yl, 0) for yh, yl in order], axis=0)
    pre_gate = jnp.dot(wg_ref[...], x_t, preferred_element_type=F32)
    pre_up = jnp.dot(wu_ref[...], x_t, preferred_element_type=F32)
    c_t = jnp.concatenate([column(rows_ref, yh, yl, 1) for yh, yl in order], axis=0)
    hid_grad = jnp.dot(wd_ref[...], c_t, preferred_element_type=F32)
    sig = jax.nn.sigmoid(pre_gate)
    act = pre_gate * sig
    hidden = (act * pre_up).astype(BF16)
    gate_part = (hid_grad * pre_up * sig * (1.0 + pre_gate * (1.0 - sig))).astype(BF16)
    up_part = (hid_grad * act).astype(BF16)
    dots = jnp.sum(hidden.astype(F32) * hid_grad, axis=0, keepdims=True)
    parts_ref[0:hid] = gate_part
    parts_ref[hid : 2 * hid] = up_part
    parts_ref[2 * hid : 3 * hid] = hidden
    parts = parts_ref[0 : 2 * hid]
    tail = dot_rows(dots).astype(BF16)
    for k, (yh, yl) in enumerate(order):
        cols = slice(k * n_x * feats, (k + 1) * n_x * feats)
        w = jnp.concatenate([wg_ref[:, cols], wu_ref[:, cols]], axis=0)
        piece = dot(w, parts, ((0,), (0,))).astype(BF16)
        for x in range(n_x):
            at = (yh * 2 + x // 2) * feats
            out_ref[around(yl, x % 2), at : at + feats] = piece[x * feats : (x + 1) * feats]
    for k in range(n_near):
        out_ref[k, n_far * feats :] = tail


def weights_body(parts_ref, rows_ref, gate_ref, up_ref, down_ref):
    n_yh = rows_ref.shape[1] * rows_ref.shape[2] // 2
    wide = 4 * (rows_ref.shape[3] // 2)
    hid = gate_ref.shape[0]
    for yh in range(n_yh):
        for yl in range(2):
            k = 2 * yh + yl
            cols = slice(k * wide, (k + 1) * wide)
            x_t, c_t = column(rows_ref, yh, yl, 0), column(rows_ref, yh, yl, 1)
            grads = dot(parts_ref[0 : 2 * hid], x_t, ((1,), (1,))).astype(BF16)
            gate_ref[:, cols] = grads[:hid]
            up_ref[:, cols] = grads[hid:]
            down_ref[:, cols] = dot(parts_ref[2 * hid :], c_t, ((1,), (1,))).astype(BF16)


def near_body(in_ref, out_ref):
    n, height, _ = in_ref.shape
    n_y, tall, _ = out_ref.shape
    feats = tall - 8
    for y in range(n_y):
        total = in_ref[0, y * feats : (y + 1) * feats].astype(F32)
        for k in range(1, n):
            total = total + in_ref[k, y * feats : (y + 1) * feats].astype(F32)
        out_ref[y, :feats] = total.astype(BF16)
    tail = in_ref[0, height - 8 :].astype(F32)
    for k in range(1, n):
        tail = tail + in_ref[k, height - 8 :].astype(F32)
    tail = dot_rows(jnp.sum(tail, axis=0, keepdims=True)).astype(BF16)
    for y in range(n_y):
        out_ref[y, feats:] = tail


def far_body(in_ref, out_ref):
    n, tall, rows = in_ref.shape
    total = in_ref[0].astype(F32)
    for k in range(1, n):
        total = total + in_ref[k].astype(F32)
    feats = tall - 8
    tail = dot_rows(jnp.sum(total[feats:], axis=0, keepdims=True))
    rest = jnp.zeros((out_ref.shape[1] - tall, rows), F32)
    whole = jnp.concatenate([total[:feats], tail, rest], axis=0)
    out_ref[...] = whole.T.astype(BF16)


def final_body(start_ref, back_ref, dest_ref, gates_ref, tokens_ref, ratio_ref):
    rows, lanes = back_ref.shape
    feats, toks = tokens_ref.shape
    top_k, share = ratio_ref.shape
    back = back_ref[...]
    dots = back[:, feats : feats + 1].astype(F32) + back[:, feats + 1 : feats + 2].astype(F32)
    place = iota((rows, toks), 0)
    select = jnp.zeros((rows, toks), F32)
    start = start_ref[0]
    for k in range(top_k):
        at = place == dest_ref[k : k + 1, :]
        select = select + jnp.where(at, 1.0, 0.0)
        mine = jnp.sum(jnp.where(at, dots, 0.0), axis=0, keepdims=True) / gates_ref[k : k + 1, :]
        for j in range(share):
            here = iota((1, toks), 1) == start + j
            ratio_ref[k : k + 1, j : j + 1] = jnp.sum(jnp.where(here, mine, 0.0), axis=1, keepdims=True)
    summed = dot(back, select.astype(BF16), ((0,), (0,)))
    tokens_ref[...] = summed[:feats].astype(BF16)


def exchange(array, axis, groups=None):
    return lax.all_to_all(
        array, axis, split_axis=0, concat_axis=0, tiled=True, axis_index_groups=groups
    )


def neighbours(n_ep, n_y, n_x):
    groups = []
    for ep in range(n_ep):
        step = 2 * (ep % 2)
        for y in range(1, n_y, 2):
            for x in range(1, n_x, 2):
                ys, xs = ((y - 1 + step) % n_y, y), ((x - 1 + step) % n_x, x)
                groups.append(circle(ys, xs, ep, n_y, n_x))
    return groups


def second_groups(n_ep, n_y, n_x):
    groups = []
    for ep in range(n_ep):
        for a in range(0, n_y, 4):
            for yl in range(2):
                ys = ((a + 4 * (ep % 2)) % n_y + yl, a + 2 + yl)
                for xl in range(2):
                    xs = (xl, xl + 2)
                    groups.append(circle(ys, xs, ep, n_y, n_x))
    return groups


def on_device(tokens, out_grad, routes, gates, gate_weight, up_weight, down_weight):
    tok_dev, top_k = routes.shape
    n_ep, n_far, n_near = lax.axis_size("ep"), lax.axis_size(FAR), 4
    whole = ("ep", *TP)
    blocks = neighbours(n_ep, lax.axis_size(("ya", "yb", "yl")), 2 * lax.axis_size("xh"))
    n_ya, n_second = lax.axis_size("ya"), lax.axis_size(SECOND)
    pairs = second_groups(n_ep, lax.axis_size(("ya", "yb", "yl")), 2 * lax.axis_size("xh"))
    cap = (3 * tok_dev + n_ep - 1) // n_ep
    rows = n_ep * cap
    feats = tokens.shape[1]
    both = 2 * feats
    w_gate, w_up, w_down = gate_weight[0].T, up_weight[0].T, down_weight[0]
    hid, width = w_gate.shape

    table = jnp.zeros((2 * feats + 2 * top_k, tok_dev), F32)
    at = 0
    for a in (tokens, out_grad, routes, gates):
        table += jnp.pad(a.T, ((at, table.shape[0] - at - a.shape[1]), (0, 0))).astype(F32)
        at += a.shape[1]
    sent, dest = call(
        functools.partial(place_body, n_ep=n_ep, cap=cap, top_k=top_k),
        [((n_ep, n_ya, cap, both), BF16), ((top_k, tok_dev), I32)],
    )(table)
    got = exchange(sent.reshape(n_ep * n_ya, cap, both), FIRST).reshape(n_ep, n_ya, cap, both)
    (copies,) = call(turn_body, [((n_second, n_ya, both, rows), BF16)])(got)
    some = exchange(copies, whole, pairs)
    every = exchange(jnp.broadcast_to(some[None], (n_near, *some.shape)), whole, blocks)

    chunks, parts = call(
        expert_body,
        [((n_near, n_far * feats + 8, rows), BF16), ((3 * hid, rows), BF16)],
        flops=10 * hid * width * rows,
        limit=20,
    )(every, w_gate, w_up, w_down)
    swapped = exchange(chunks, whole, blocks)
    gate_grad, up_grad, down_grad = call(
        weights_body, [((hid, width), BF16)] * 3, flops=6 * hid * width * rows, limit=60
    )(parts, every)
    (near,) = call(near_body, [((n_far, feats + 8, rows), BF16)])(swapped)
    (packed,) = call(far_body, [((rows, both), BF16)])(exchange(near, FAR))
    back = exchange(packed.reshape(n_ep, cap, both), "ep").reshape(rows, both)
    share = tok_dev // (n_far * n_near)
    start = (lax.axis_index(TP).astype(I32) * share).reshape(1)
    tokens_grad, ratio = call(
        final_body, [((feats, tok_dev), BF16), ((top_k, share), F32)], n_scalars=1
    )(start, back, dest, gates.T)
    return (
        tokens_grad.T,
        ratio.T,
        gate_grad.T[None],
        up_grad.T[None],
        down_grad[None],
    )


def solution(mesh):
    torus = Mesh(mesh.devices.reshape(mesh.shape["ep"], 2, 2, 2, 2, 2), ("ep", *TP))
    return jax.shard_map(
        on_device,
        mesh=torus,
        in_specs=(
            P("ep", TP),
            P("ep", TP),
            P("ep", None),
            P("ep", None),
            P("ep", None, TP),
            P("ep", None, TP),
            P("ep", TP, None),
        ),
        out_specs=(
            P("ep", TP),
            P(("ep", *TP), None),
            P("ep", None, TP),
            P("ep", None, TP),
            P("ep", TP, None),
        ),
        check_vma=False,
    )
```
